32 devices in a mesh: sp: 8 (over z, y), tp: 4 (over x, core).
Axes of the slice: x: 2, y: 2, z: 4, core: 2. Of those that a mesh axis runs over, the one named last changes fastest.
Arguments:
- tokens: bfloat16 [2048, 2048], P(('sp', 'tp')), may hold values from -6 to 6
- pre_gain: float32 [2048], replicated, may hold values from 0.1 to 1.9
- w_query_ret: bfloat16 [2048, 768], P('sp', 'tp'), may hold values from -0.125 to 0.125
- w_key_ret: bfloat16 [2048, 768], P('sp', 'tp'), may hold values from -0.125 to 0.125
- w_value_ret: bfloat16 [2048, 768], P('sp', 'tp'), may hold values from -0.125 to 0.125
- w_query_att: bfloat16 [2048, 768], P('sp', 'tp'), may hold values from -0.5 to 0.5
- w_key_att: bfloat16 [2048, 256], P('sp', 'tp'), may hold values from -0.125 to 0.125
- w_value_att: bfloat16 [2048, 256], P('sp', 'tp'), may hold values from -0.125 to 0.125
- w_out_ret: bfloat16 [768, 2048], P('tp', 'sp'), may hold values from -0.15625 to 0.15625
- w_out_att: bfloat16 [768, 2048], P('tp', 'sp'), may hold values from -0.15625 to 0.15625
- retain_log: float32 [2048, 12], P('sp', 'tp')
- forget_total: float32 [12, 2048], P('tp'), as said below
Outputs:
- mixed: bfloat16 [2048, 2048], P(('sp', 'tp'))
The draws below stay inside these ranges and needn't reach their ends.
Inputs may be any that keep to these rules, and one draw needn't show every extreme that they name: `forget_total`: never rises along positions.
All inputs are finite; a program needn't handle non-finite values.
Results may differ from the reference program's by a relative error of at most 0.019.
Values may be sent and summed in bfloat16 or wider, within the bound.
A program may use at most 64 MiB of HBM per device.

```python
import math
import jax
import jax.numpy as jnp
from jax import lax

D = 2048
HEAD = 64
R_HEADS = 12
F_HEADS = 12
KV_HEADS = 4
SPAN = 256
TOK_DEV = 256
TOKENS = 2048
N_TP = 4


def log_rates(key, heads):
    keys = jax.random.split(key, 6)
    order = jax.random.permutation(keys[0], heads)
    slow = order < heads // 2
    blocks = TOKENS // TOK_DEV
    spread = jnp.exp(jax.random.uniform(keys[1], (blocks, heads), jnp.float32, math.log(0.4), math.log(2.5)))
    spread = jnp.repeat(spread, TOK_DEV, axis=0)
    rough = jax.random.uniform(keys[2], (TOKENS, heads), jnp.float32, 0.5, 1.5)
    fast = jnp.exp(jax.random.uniform(keys[3], (heads,), jnp.float32, math.log(0.03), math.log(0.1)))
    base = jnp.where(slow, 0.2 * math.log(10.0) / TOKENS, fast)
    rates = base[None, :] * spread * rough
    places = jax.random.randint(keys[4], (2, heads), 0, TOKENS)
    losses = jax.random.uniform(keys[5], (2, heads), jnp.float32, 0.2, 0.4)
    struck = jnp.arange(TOKENS, dtype=jnp.int32)[:, None, None] == places[None, :, :]
    rates = rates - jnp.sum(jnp.where(struck, jnp.log(1.0 - losses)[None, :, :], 0.0), axis=1)
    return -rates


def draw_retain_log(key, part):
    return log_rates(jax.random.fold_in(key, 11), R_HEADS)


def draw_forget_total(key, part):
    return jnp.transpose(jnp.cumsum(log_rates(jax.random.fold_in(key, 23), F_HEADS), axis=0))


def block_levels(own_key, extent, cuts, least, high):
    factor_of, own = 1.0, jax.random.fold_in(own_key, 6)
    for dim, shards_of in cuts:
        heights = jnp.exp(jax.random.uniform(jax.random.fold_in(own, dim), (shards_of,), jnp.float32, least / len(cuts), high / len(cuts)))
        factor_of = factor_of * jnp.repeat(heights, extent[dim] // shards_of).reshape([-1 if axis == dim else 1 for axis in range(len(extent))])
    return factor_of


def scatter_about(stream_key, dims, deviation, reach, cuts=(), kind=jnp.bfloat16):
    values = deviation * jax.random.normal(stream_key, dims, jnp.float32)
    if cuts:
        values = values * block_levels(stream_key, dims, cuts, -0.22, 0.18)
    return jnp.clip(values, -reach, reach).astype(kind)


def setup_inputs(seed: int = 0) -> dict:
    seeds = jax.random.split(jax.random.key(seed), 13)
    tokens = scatter_about(seeds[0], (TOKENS, D), 1.0, 6.0, ((0, 32),))
    pre_gain = jnp.clip(1.0 + 0.18 * jax.random.normal(seeds[1], (D,), jnp.float32), 0.1, 1.9)
    w_query_ret = scatter_about(seeds[2], (D, R_HEADS * HEAD), D ** -0.5, 0.125, ((0, 8), (1, 4)))
    w_key_ret = scatter_about(seeds[3], (D, R_HEADS * HEAD), D ** -0.5, 0.125, ((0, 8), (1, 4)))
    w_value_ret = scatter_about(seeds[4], (D, R_HEADS * HEAD), D ** -0.5, 0.125, ((0, 8), (1, 4)))
    w_query_att = scatter_about(seeds[5], (D, F_HEADS * HEAD), (D // 16) ** -0.5, 0.5, ((0, 8), (1, 4)))
    w_key_att = scatter_about(seeds[6], (D, KV_HEADS * HEAD), D ** -0.5, 0.125, ((0, 8), (1, 4)))
    w_value_att = scatter_about(seeds[7], (D, KV_HEADS * HEAD), D ** -0.5, 0.125, ((0, 8), (1, 4)))
    w_out_ret = scatter_about(seeds[8], (R_HEADS * HEAD, D), (2 * R_HEADS * HEAD) ** -0.5, 0.15625, ((0, 4), (1, 8)))
    w_out_att = scatter_about(seeds[9], (F_HEADS * HEAD, D), (2 * F_HEADS * HEAD) ** -0.5, 0.15625, ((0, 4), (1, 8)))
    retain_log = draw_retain_log(jax.random.fold_in(seeds[12], 71), 0)
    forget_total = draw_forget_total(jax.random.fold_in(seeds[12], 71), 0)
    return dict(tokens=tokens, pre_gain=pre_gain, w_query_ret=w_query_ret, w_key_ret=w_key_ret, w_value_ret=w_value_ret, w_query_att=w_query_att, w_key_att=w_key_att, w_value_att=w_value_att, w_out_ret=w_out_ret, w_out_att=w_out_att, retain_log=retain_log, forget_total=forget_total)


EPS = 1e-06
THETA = 10000.0

def rotate(field, positions):
    half = field.shape[-1] // 2
    inverse = THETA ** (-jnp.arange(half, dtype=jnp.float32) / half)
    angles = positions[:, None] * inverse[None, :]
    cosine = jnp.cos(angles)[:, None, :]
    sine = jnp.sin(angles)[:, None, :]
    first_half = field[..., :half]
    second_half = field[..., half:]
    return jnp.concatenate([first_half * cosine - second_half * sine, first_half * sine + second_half * cosine], axis=-1)

def head_norm(values):
    centre = lax.optimization_barrier(jnp.mean(values, axis=-1, keepdims=True))
    spread = lax.optimization_barrier(jnp.mean(jnp.square(values - centre), axis=-1, keepdims=True))
    return (values - centre) * lax.rsqrt(spread + EPS)

def lowered(values):
    return lax.optimization_barrier(values.astype(jnp.bfloat16)).astype(jnp.float32)

def retain_block(state, inputs):
    query, key_rows, value_rows, logs = inputs
    within = jnp.cumsum(logs, axis=0)
    span = logs.shape[0]
    causal = jnp.arange(span)[:, None] >= jnp.arange(span)[None, :]
    scores = jnp.einsum('thd,shd->hts', query.astype(jnp.float32), key_rows.astype(jnp.float32))
    gap = jnp.where(causal, jnp.transpose(within)[:, :, None] - jnp.transpose(within)[:, None, :], 0.0)
    weights = jnp.where(causal, scores * jnp.exp(gap), 0.0).astype(jnp.bfloat16)
    local = jnp.einsum('hts,shd->thd', weights.astype(jnp.float32), value_rows.astype(jnp.float32))
    lifted = lowered(query.astype(jnp.float32) * jnp.exp(within)[:, :, None])
    carried = jnp.einsum('thd,hde->the', lifted, lowered(state))
    last = within[-1]
    faded = lowered(key_rows.astype(jnp.float32) * jnp.exp(last[None, :] - within)[:, :, None])
    update = jnp.einsum('shd,she->hde', faded, value_rows.astype(jnp.float32))
    return (jnp.exp(last)[:, None, None] * state + update, local + carried)

def project(normed, weight):
    return jnp.dot(normed, weight, preferred_element_type=jnp.float32)

def reference(tokens, pre_gain, w_query_ret, w_key_ret, w_value_ret, w_query_att, w_key_att, w_value_att, w_out_ret, w_out_att, retain_log, forget_total):
    rows = tokens.astype(jnp.float32)
    normed = (rows * lax.rsqrt(lax.optimization_barrier(jnp.mean(rows * rows, axis=-1, keepdims=True)) + EPS) * pre_gain.astype(jnp.float32)).astype(jnp.bfloat16)
    positions = jnp.arange(TOKENS, dtype=jnp.int32).astype(jnp.float32)
    shape = (TOKENS, R_HEADS, HEAD)
    ret_query = (rotate(project(normed, w_query_ret).reshape(shape), positions) * HEAD ** (-0.5)).astype(jnp.bfloat16)
    ret_key = rotate(project(normed, w_key_ret).reshape(shape), positions).astype(jnp.bfloat16)
    ret_value = project(normed, w_value_ret).astype(jnp.bfloat16).reshape(shape)
    blocks = TOKENS // SPAN
    start_state = jnp.zeros((R_HEADS, HEAD, HEAD), jnp.float32)
    inputs = (ret_query.reshape(blocks, SPAN, R_HEADS, HEAD), ret_key.reshape(blocks, SPAN, R_HEADS, HEAD), ret_value.reshape(blocks, SPAN, R_HEADS, HEAD), retain_log.reshape(blocks, SPAN, R_HEADS))
    _, inside = lax.scan(retain_block, start_state, inputs)
    retained = head_norm(inside.reshape(shape)).astype(jnp.bfloat16).reshape(TOKENS, R_HEADS * HEAD)
    group = F_HEADS // KV_HEADS
    pieces = TOKENS // TOK_DEV
    att_query = (project(normed, w_query_att) * HEAD ** (-0.5)).astype(jnp.bfloat16).reshape(pieces, TOK_DEV, KV_HEADS, group, HEAD)
    att_key = project(normed, w_key_att).astype(jnp.bfloat16).reshape(pieces, TOK_DEV, KV_HEADS, HEAD)
    att_value = project(normed, w_value_att).astype(jnp.bfloat16).reshape(pieces, TOK_DEV, KV_HEADS, HEAD)
    gates = forget_total.reshape(KV_HEADS, group, pieces, TOK_DEV)
    local_places = jnp.arange(TOK_DEV, dtype=jnp.int32)

    def attend_block(index):
        query_rows = lax.dynamic_index_in_dim(att_query, index, 0, keepdims=False).astype(jnp.float32)
        gate_rows = lax.dynamic_index_in_dim(gates, index, 2, keepdims=False)
        query_places = index * TOK_DEV + local_places

        def add_keys(other, carry):
            weighted, total = carry
            key_rows = lax.dynamic_index_in_dim(att_key, other, 0, keepdims=False).astype(jnp.float32)
            value_rows = lax.dynamic_index_in_dim(att_value, other, 0, keepdims=False).astype(jnp.float32)
            gate_keys = lax.dynamic_index_in_dim(gates, other, 2, keepdims=False)
            scores = jnp.einsum('tcgd,scd->cgts', query_rows, key_rows)
            logits = scores + gate_rows[:, :, :, None] - gate_keys[:, :, None, :]
            allowed = (other * TOK_DEV + local_places)[None, :] <= query_places[:, None]
            weights = jnp.exp(jnp.where(allowed, logits, -jnp.inf))
            total = total + lax.optimization_barrier(jnp.sum(weights, axis=-1))
            weighted = weighted + jnp.einsum('cgts,scd->cgtd', weights.astype(jnp.bfloat16).astype(jnp.float32), value_rows)
            return (weighted, total)
        init = (jnp.zeros((KV_HEADS, group, TOK_DEV, HEAD), jnp.float32), jnp.zeros((KV_HEADS, group, TOK_DEV), jnp.float32))
        weighted, total = lax.fori_loop(0, index + 1, add_keys, init)
        return (weighted / total[..., None]).astype(jnp.bfloat16)
    outputs = lax.map(attend_block, jnp.arange(pieces, dtype=jnp.int32))
    attended = jnp.transpose(outputs, (0, 3, 1, 2, 4)).reshape(TOKENS, F_HEADS * HEAD)
    ret_width = R_HEADS // N_TP * HEAD
    att_width = F_HEADS // N_TP * HEAD
    summed = jnp.zeros((TOKENS, D), jnp.float32)
    for part in range(N_TP):
        term = jnp.dot(retained[:, part * ret_width:(part + 1) * ret_width], w_out_ret[part * ret_width:(part + 1) * ret_width], preferred_element_type=jnp.float32)
        term = term + jnp.dot(attended[:, part * att_width:(part + 1) * att_width], w_out_att[part * att_width:(part + 1) * att_width], preferred_element_type=jnp.float32)
        summed = summed + lax.optimization_barrier(term.astype(jnp.bfloat16)).astype(jnp.float32)
    return summed.astype(jnp.bfloat16)
```

```python
import functools

import jax
import jax.numpy as jnp
from jax import lax
from jax.experimental import pallas as pl
from jax.experimental.pallas import tpu as pltpu
from jax.sharding import PartitionSpec as P

HEAD = 64
EPS = 1e-06
THETA = 10000.0
F32 = jnp.float32
BF16 = jnp.bfloat16
MESH = pl.DeviceIdType.MESH
SPAN = 256
KEY_SPAN = 256
LANES = 128
HIGH = lax.Precision.HIGHEST


def ring_to_sp(place, n):
    if n % 2:
        return place
    back = place // (n // 2)
    return (1 - back) * 2 * place + back * (2 * (n - 1 - place) + 1)


def sp_to_ring(index, n):
    if n % 2:
        return index
    odd, pair = index % 2, index // 2
    return (1 - odd) * pair + odd * (n - 1 - pair)


def dot(a, b, dims=((1,), (0,))):
    return lax.dot_general(a, b, (dims, ((), ())), preferred_element_type=F32)


def kernel(
    n,
    m,
    heads,
    chunks,
    tok_ref,
    gain_ref,
    wa_ref,
    wb_ref,
    wo_ref,
    cos_ref,
    sin_ref,
    within_ref,
    turned_ref,
    gate_col_ref,
    gate_ref,
    out_ref,
    xbuf,
    abuf,
    bbuf,
    obuf,
    kvbuf,
    state,
    num,
    den,
    outbuf,
    rsbuf,
    *sems,
):
    (x_send, x_recv, a_send, a_recv, b_send, b_recv, o_send, o_recv, kv_send, kv_recv, r_send,
     r_recv) = sems
    me = lax.axis_index("sp")
    mine = lax.axis_index("tp")
    place = sp_to_ring(me, n)
    right = ring_to_sp((place + 1) % n, n)
    left = ring_to_sp((place + n - 1) % n, n)
    tok = xbuf.shape[0]
    rows = tok // m
    width = heads * HEAD

    barrier = pltpu.get_barrier_semaphore()
    for r in range(1, n):
        pl.semaphore_signal(barrier, inc=1, device_id={"sp": (me + r) % n}, device_id_type=MESH)
    for r in range(1, m):
        pl.semaphore_signal(barrier, inc=1, device_id={"tp": (mine + r) % m}, device_id_type=MESH)

    abuf[me] = wa_ref[...]
    bbuf[me] = wb_ref[...]
    obuf[me] = wo_ref[...]
    values = tok_ref[...].astype(F32)
    scale = lax.rsqrt(jnp.mean(values * values, axis=-1, keepdims=True) + EPS)
    own = pl.ds(mine * rows, rows)
    xbuf[own, :] = (values * scale * gain_ref[...]).astype(BF16)
    pl.semaphore_wait(barrier, n - 1 + m - 1)

    def ring_copy(own_ref, buf, send, recv, step, way, chunk):
        owner = ring_to_sp((place + (n - step if way == 0 else step)) % n, n)
        half = buf.shape[1] // 2
        piece = half // chunks
        span = pl.ds(way * half + chunk * piece, piece)
        source = own_ref.at[span] if step == 0 else buf.at[owner, span]
        return pltpu.make_async_remote_copy(
            src_ref=source,
            dst_ref=buf.at[owner, span],
            send_sem=send.at[way, step, chunk],
            recv_sem=recv.at[way, step, chunk],
            device_id={"sp": right if way == 0 else left},
            device_id_type=MESH,
        )

    def ring_wait(own_ref, buf, send, recv, step, way, chunk):
        source = ring_to_sp((place + (n - step - 1 if way == 0 else step + 1)) % n, n)
        half = buf.shape[1] // 2
        piece = half // chunks
        span = pl.ds(way * half + chunk * piece, piece)
        pltpu.make_async_remote_copy(
            src_ref=buf.at[source, span],
            dst_ref=buf.at[source, span],
            send_sem=send.at[way, step, chunk],
            recv_sem=recv.at[way, step, chunk],
            device_id={"sp": right if way == 0 else left},
            device_id_type=MESH,
        ).wait_recv()

    started = []

    def ring_step(group, step):
        for chunk in range(chunks):
            for way in range(2):
                if step > 0:
                    ring_wait(*group, step - 1, way, chunk)
                if step < n - 1:
                    copy = ring_copy(*group, step, way, chunk)
                    copy.start()
                    started.append(copy)

    ring_a = (wa_ref, abuf, a_send, a_recv)
    ring_b = (wb_ref, bbuf, b_send, b_recv)
    ring_o = (wo_ref, obuf, o_send, o_recv)

    x_copies = []
    for r in range(1, m):
        copy = pltpu.make_async_remote_copy(
            src_ref=xbuf.at[own],
            dst_ref=xbuf.at[own],
            send_sem=x_send.at[r - 1],
            recv_sem=x_recv.at[r - 1],
            device_id={"tp": (mine + r) % m},
            device_id_type=MESH,
        )
        copy.start()
        started.append(copy)
    for step in range(n - 1):
        ring_step(ring_a, step)
    ring_step(ring_b, 0)
    for r in range(1, m):
        other = pl.ds(((mine + m - r) % m) * rows, rows)
        pltpu.make_async_remote_copy(
            src_ref=xbuf.at[other],
            dst_ref=xbuf.at[other],
            send_sem=x_send.at[r - 1],
            recv_sem=x_recv.at[r - 1],
            device_id={"tp": (mine + r) % m},
            device_id_type=MESH,
        ).wait_recv()
    ring_step(ring_a, n - 1)

    cosine, sine = cos_ref[...], sin_ref[...]

    def rope(field):
        half = HEAD // 2
        first, second = field[:, :half], field[:, half:]
        return jnp.concatenate(
            [first * cosine - second * sine, first * sine + second * cosine], axis=-1
        )

    proj = dot(xbuf[...], abuf[...].reshape(-1, abuf.shape[2]))
    pair = proj[:, : 2 * HEAD].astype(BF16)
    within = within_ref[...]
    keys, vals, updates, marks = [], [], [], []
    for h in range(heads):
        base = 2 * HEAD + h * HEAD
        key = rope(proj[:, base : base + HEAD]).astype(BF16)
        val = proj[:, base + width : base + width + HEAD].astype(BF16)
        column = within[:, h : h + 1]
        last = column[tok - 1 :, :]
        faded = (key.astype(F32) * jnp.exp(last - column)).astype(BF16)
        updates.append(dot(faded, val, ((0,), (0,))))
        high = last.astype(BF16).astype(F32)
        low = last - high
        marks.append(jnp.broadcast_to(high, (8, HEAD)))
        marks.append(jnp.broadcast_to(low, (8, HEAD)))
        keys.append(key)
        vals.append(val)
    kvbuf[me, :tok, :] = pair
    for h in range(heads):
        kvbuf[me, tok + h * HEAD : tok + (h + 1) * HEAD, :HEAD] = updates[h].astype(BF16)
    kvbuf[me, tok : tok + 16 * heads, HEAD:] = jnp.concatenate(marks, axis=0).astype(BF16)
    for d in range(1, n):
        def send_kv(d=d):
            pltpu.make_async_remote_copy(
                src_ref=kvbuf.at[me],
                dst_ref=kvbuf.at[me],
                send_sem=kv_send.at[d],
                recv_sem=kv_recv.at[me],
                device_id={"sp": jnp.int32(d)},
                device_id_type=MESH,
            ).start()

        pl.when(me < d)(send_kv)

    for step in range(1, n - 1):
        ring_step(ring_b, step)
    ring_step(ring_o, 0)
    ring_step(ring_b, n - 1)

    projq = dot(xbuf[...], bbuf[...].reshape(-1, bbuf.shape[2]))
    ring_step(ring_o, 1)
    lines = lax.broadcasted_iota(jnp.int32, (tok, tok), 0)
    across = lax.broadcasted_iota(jnp.int32, (tok, tok), 1)
    causal = lines >= across
    turned = turned_ref[...]
    local, lifts = [], []
    for h in range(heads):
        base = width + h * HEAD
        query = (rope(projq[:, base : base + HEAD]) * HEAD ** (-0.5)).astype(BF16)
        column = within[:, h : h + 1]
        gap = jnp.where(causal, column - turned[h : h + 1, :], 0.0)
        scores = dot(query, keys[h], ((1,), (1,)))
        weights = jnp.where(causal, scores * jnp.exp(gap), 0.0).astype(BF16)
        local.append(dot(weights, vals[h]))
        lifts.append((query.astype(F32) * jnp.exp(column)).astype(BF16))
    ring_step(ring_o, 2)

    queries = [
        (projq[:, h * HEAD : (h + 1) * HEAD] * HEAD ** (-0.5)).astype(BF16) for h in range(heads)
    ]
    gate_col = gate_col_ref[...]

    def attend(index, masked):
        block = kvbuf[index, :tok, :]
        key, val = block[:, :HEAD], block[:, HEAD:]
        gates = gate_ref[:, pl.ds(pl.multiple_of(index * tok, tok), tok)]
        for h in range(heads):
            logits = dot(queries[h], key, ((1,), (1,)))
            logits = logits + gate_col[:, h : h + 1] - gates[h : h + 1, :]
            if masked:
                logits = jnp.where(causal, logits, -jnp.inf)
            weights = jnp.exp(logits)
            den[h] += jnp.broadcast_to(jnp.sum(weights, axis=-1, keepdims=True), (tok, HEAD))
            num[h] += dot(weights.astype(BF16), val)

    den[...] = jnp.zeros_like(den)
    num[...] = jnp.zeros_like(num)
    state[...] = jnp.zeros_like(state)
    attend(me, True)
    for j in range(n - 1):
        def earlier(j=j):
            pltpu.make_async_remote_copy(
                src_ref=kvbuf.at[j],
                dst_ref=kvbuf.at[j],
                send_sem=kv_send.at[0],
                recv_sem=kv_recv.at[j],
                device_id={"sp": right},
                device_id_type=MESH,
            ).wait_recv()
            for h in range(heads):
                mark = kvbuf[j, tok + 16 * h : tok + 16 * (h + 1), HEAD:].astype(F32)
                total = mark[0:1] + mark[8:9]
                new = kvbuf[j, tok + h * HEAD : tok + (h + 1) * HEAD, :HEAD].astype(F32)
                state[h] = jnp.exp(total) * state[h] + new
            attend(jnp.int32(j), False)

        pl.when(me > j)(earlier)
        if 3 + j <= n - 1:
            ring_step(ring_o, 3 + j)
    for step in range(3 + n - 1, n):
        ring_step(ring_o, step)

    retained, attended = [], []
    for h in range(heads):
        raw = local[h] + dot(lifts[h], state[h].astype(BF16))
        centre = jnp.mean(raw, axis=-1, keepdims=True)
        spread = jnp.mean(jnp.square(raw - centre), axis=-1, keepdims=True)
        retained.append(((raw - centre) * lax.rsqrt(spread + EPS)).astype(BF16))
        attended.append((num[h] / den[h]).astype(BF16))
    mixed = jnp.concatenate(retained + attended, axis=-1)

    def out_copy(r, part, span):
        return pltpu.make_async_remote_copy(
            src_ref=outbuf.at[(mine + r) % m, :, span],
            dst_ref=rsbuf.at[mine, :, span],
            send_sem=r_send.at[r - 1, part],
            recv_sem=r_recv.at[r - 1, part],
            device_id={"tp": (mine + r) % m},
            device_id_type=MESH,
        )

    columns = obuf.shape[2]
    group = 2 if n % 2 == 0 else 1
    for part in range(n // group):
        for k in range(part * group, part * group + group):
            share = dot(mixed, obuf[k]).astype(BF16)
            outbuf[:, :, k * columns : (k + 1) * columns] = share.reshape(m, rows, columns)
        span = pl.ds(part * group * columns, group * columns)
        for r in range(1, m):
            copy = out_copy(r, part, span)
            copy.start()
            started.append(copy)
    for part in range(n // group):
        span = pl.ds(part * group * columns, group * columns)
        total = outbuf[mine, :, span].astype(F32)
        for r in range(1, m):
            other = (mine + m - r) % m
            pltpu.make_async_remote_copy(
                src_ref=rsbuf.at[other, :, span],
                dst_ref=rsbuf.at[other, :, span],
                send_sem=r_send.at[r - 1, part],
                recv_sem=r_recv.at[r - 1, part],
                device_id={"tp": (mine + r) % m},
                device_id_type=MESH,
            ).wait_recv()
            total = total + rsbuf[other, :, span].astype(F32)
        out_ref[:, span] = total.astype(BF16)

    for copy in started:
        copy.wait_send()
    for d in range(1, n):
        def sent(d=d):
            pltpu.make_async_remote_copy(
                src_ref=kvbuf.at[me],
                dst_ref=kvbuf.at[me],
                send_sem=kv_send.at[d],
                recv_sem=kv_recv.at[me],
                device_id={"sp": jnp.int32(d)},
                device_id_type=MESH,
            ).wait_send()

        pl.when(me < d)(sent)


def body(
    n,
    m,
    tokens,
    pre_gain,
    w_query_ret,
    w_key_ret,
    w_value_ret,
    w_query_att,
    w_key_att,
    w_value_att,
    w_out_ret,
    w_out_att,
    retain_log,
    forget_total,
):
    rows, depth = tokens.shape
    tok = rows * m
    heads = retain_log.shape[1]
    offset = lax.axis_index("sp") * tok
    wa = jnp.concatenate([w_key_att, w_value_att, w_key_ret, w_value_ret], axis=1)
    wb = jnp.concatenate([w_query_att, w_query_ret], axis=1)
    wo = jnp.concatenate([w_out_ret, w_out_att], axis=0)
    half = HEAD // 2
    positions = (offset + jnp.arange(tok, dtype=jnp.int32)).astype(F32)
    inverse = THETA ** (-jnp.arange(half, dtype=F32) / half)
    angles = positions[:, None] * inverse[None, :]
    within = jnp.cumsum(retain_log, axis=0)
    gate_col = lax.dynamic_slice_in_dim(forget_total, offset, tok, 1).T
    chunks = 4
    vmem = pl.BlockSpec(memory_space=pltpu.VMEM)
    dma = pltpu.SemaphoreType.DMA
    rings = [dma((2, n - 1, chunks))] * 6
    parts = n // 2 if n % 2 == 0 else n
    return pl.pallas_call(
        functools.partial(kernel, n, m, heads, chunks),
        out_shape=jax.ShapeDtypeStruct((rows, depth), BF16),
        in_specs=[vmem] * 11,
        out_specs=vmem,
        scratch_shapes=[
            pltpu.VMEM((tok, depth), BF16),
            pltpu.VMEM((n,) + wa.shape, BF16),
            pltpu.VMEM((n,) + wb.shape, BF16),
            pltpu.VMEM((n,) + wo.shape, BF16),
            pltpu.VMEM((n, tok + heads * HEAD, 2 * HEAD), BF16),
            pltpu.VMEM((heads, HEAD, HEAD), F32),
            pltpu.VMEM((heads, tok, HEAD), F32),
            pltpu.VMEM((heads, tok, HEAD), F32),
            pltpu.VMEM((m, rows, depth), BF16),
            pltpu.VMEM((m, rows, depth), BF16),
            dma((m - 1,)),
            dma((m - 1,)),
            *rings,
            dma((n,)),
            dma((n,)),
            dma((m - 1, parts)),
            dma((m - 1, parts)),
        ],
        compiler_params=pltpu.CompilerParams(
            collective_id=0, has_side_effects=True, vmem_limit_bytes=60 * 1024 * 1024
        ),
    )(
        tokens,
        pre_gain[None, :],
        wa,
        wb,
        wo,
        jnp.cos(angles),
        jnp.sin(angles),
        within,
        within.T,
        gate_col,
        forget_total,
    )


def rotate(field, positions):
    half = field.shape[-1] // 2
    inverse = THETA ** (-jnp.arange(half, dtype=jnp.float32) / half)
    angles = positions[:, None] * inverse[None, :]
    cosine = jnp.cos(angles)[:, None, :]
    sine = jnp.sin(angles)[:, None, :]
    first_half = field[..., :half]
    second_half = field[..., half:]
    return jnp.concatenate(
        [first_half * cosine - second_half * sine, first_half * sine + second_half * cosine],
        axis=-1,
    )


def head_norm(values):
    centre = jnp.mean(values, axis=-1, keepdims=True)
    spread = jnp.mean(jnp.square(values - centre), axis=-1, keepdims=True)
    return (values - centre) * lax.rsqrt(spread + EPS)


def advance(state, pair):
    decay, update = pair
    return (jnp.exp(decay)[:, None, None] * state + update, state)


def plain_body(
    tokens,
    pre_gain,
    w_query_ret,
    w_key_ret,
    w_value_ret,
    w_query_att,
    w_key_att,
    w_value_att,
    w_out_ret,
    w_out_att,
    retain_log,
    forget_total,
):
    rows = tokens.astype(jnp.float32)
    normed = (
        rows * lax.rsqrt(jnp.mean(rows * rows, axis=-1, keepdims=True) + EPS) * pre_gain
    ).astype(jnp.bfloat16)
    gathered = lax.all_gather(normed, "tp", axis=0, tiled=True)
    tok_dev = gathered.shape[0]
    offset = lax.axis_index("sp") * tok_dev
    query_places = offset + jnp.arange(tok_dev, dtype=jnp.int32)
    positions = query_places.astype(jnp.float32)

    def blocked(values):
        return values.reshape((tok_dev // SPAN, SPAN) + values.shape[1:])

    pieces = (
        lax.all_gather(w_query_ret, "sp", axis=0, tiled=True),
        lax.all_gather(w_key_ret, "sp", axis=0, tiled=True),
        lax.all_gather(w_value_ret, "sp", axis=0, tiled=True),
        lax.all_gather(w_query_att, "sp", axis=0, tiled=True),
        lax.all_gather(w_key_att, "sp", axis=0, tiled=True),
        lax.all_gather(w_value_att, "sp", axis=0, tiled=True),
    )
    projected = tuple(
        (jnp.dot(gathered, piece, preferred_element_type=jnp.float32) for piece in pieces)
    )
    heads = retain_log.shape[1]
    shape = (tok_dev, heads, HEAD)
    query = blocked(
        (rotate(projected[0].reshape(shape), positions) * HEAD ** (-0.5)).astype(jnp.bfloat16)
    )
    key_rows = blocked(rotate(projected[1].reshape(shape), positions).astype(jnp.bfloat16))
    value_rows = blocked(projected[2].astype(jnp.bfloat16).reshape(shape))
    within = jnp.cumsum(blocked(retain_log), axis=1)
    causal = jnp.arange(SPAN)[:, None] >= jnp.arange(SPAN)[None, :]
    scores = jnp.einsum("bthd,bshd->bhts", query, key_rows, preferred_element_type=jnp.float32)
    turned = jnp.transpose(within, (0, 2, 1))
    gap = jnp.where(causal, turned[:, :, :, None] - turned[:, :, None, :], 0.0)
    weights = jnp.where(causal, scores * jnp.exp(gap), 0.0).astype(jnp.bfloat16)
    local = jnp.einsum("bhts,bshd->bthd", weights, value_rows, preferred_element_type=jnp.float32)
    last = within[:, -1]
    faded = (key_rows.astype(jnp.float32) * jnp.exp(last[:, None, :] - within)[..., None]).astype(
        jnp.bfloat16
    )
    updates = jnp.einsum("bshd,bshe->bhde", faded, value_rows, preferred_element_type=jnp.float32)
    zero_state = jnp.zeros((heads, HEAD, HEAD), jnp.float32)
    final, _ = lax.scan(advance, zero_state, (last, updates))
    decay_total = jnp.sum(last, axis=0)
    own_state = final.reshape(heads, HEAD * HEAD)
    every_total = lax.all_gather(
        decay_total[None].astype(jnp.bfloat16), "sp", axis=0, tiled=True
    ).astype(jnp.float32)
    every_state = lax.all_gather(
        own_state[None].astype(jnp.bfloat16), "sp", axis=0, tiled=True
    ).astype(jnp.float32)
    device_order = jnp.arange(every_total.shape[0], dtype=jnp.int32)[:, None]
    earlier = device_order < lax.axis_index("sp")
    before = jnp.sum(jnp.where(earlier, every_total, 0.0), axis=0)
    through = jnp.cumsum(every_total, axis=0)
    fading = jnp.where(earlier, jnp.exp(jnp.where(earlier, before[None, :] - through, 0.0)), 0.0)
    incoming = jnp.einsum("jh,jhe->he", fading, every_state, precision=HIGH)
    _, befores = lax.scan(advance, incoming.reshape(heads, HEAD, HEAD), (last, updates))
    lifted = (query.astype(jnp.float32) * jnp.exp(within)[..., None]).astype(jnp.bfloat16)
    carried = jnp.einsum(
        "bthd,bhde->bthe", lifted, befores.astype(jnp.bfloat16), preferred_element_type=jnp.float32
    )
    retained = (
        head_norm((local + carried).reshape(shape))
        .astype(jnp.bfloat16)
        .reshape(tok_dev, heads * HEAD)
    )
    raw_key = projected[4]
    gate_heads = forget_total.shape[0]
    kv_local = raw_key.shape[1] // HEAD
    group = gate_heads // kv_local
    query = (
        (projected[3] * HEAD ** (-0.5)).astype(jnp.bfloat16).reshape(tok_dev, kv_local, group, HEAD)
    )
    key_rows = raw_key.astype(jnp.bfloat16)
    value_rows = projected[5].astype(jnp.bfloat16)
    gate_rows = lax.dynamic_slice_in_dim(forget_total, offset, tok_dev, 1).reshape(
        kv_local, group, tok_dev
    )
    last_row = offset + tok_dev - 1
    init = (
        jnp.zeros((kv_local, group, tok_dev, HEAD), jnp.float32),
        jnp.zeros((kv_local, group, tok_dev), jnp.float32),
    )
    key_piece = lax.all_gather(key_rows, "sp", axis=0, tiled=True)
    value_piece = lax.all_gather(value_rows, "sp", axis=0, tiled=True)
    count = key_piece.shape[0] // KEY_SPAN

    def one_block(index, inner):
        first = index * KEY_SPAN

        def compute(state):
            weighted, total = state
            key_block = lax.dynamic_slice_in_dim(key_piece, index * KEY_SPAN, KEY_SPAN, 0).reshape(
                KEY_SPAN, kv_local, HEAD
            )
            value_block = lax.dynamic_slice_in_dim(
                value_piece, index * KEY_SPAN, KEY_SPAN, 0
            ).reshape(KEY_SPAN, kv_local, HEAD)
            gate_keys = lax.dynamic_slice_in_dim(forget_total, first, KEY_SPAN, 1).reshape(
                kv_local, group, KEY_SPAN
            )
            scores = jnp.einsum(
                "tcgd,scd->cgts", query, key_block, preferred_element_type=jnp.float32
            )
            logits = scores + gate_rows[:, :, :, None] - gate_keys[:, :, None, :]
            allowed = (first + jnp.arange(KEY_SPAN, dtype=jnp.int32))[None, :] <= query_places[
                :, None
            ]
            weights = jnp.exp(jnp.where(allowed, logits, -jnp.inf))
            total = total + jnp.sum(weights, axis=-1)
            weighted = weighted + jnp.einsum(
                "cgts,scd->cgtd",
                weights.astype(jnp.bfloat16),
                value_block,
                preferred_element_type=jnp.float32,
            )
            return (weighted, total)

        def skipped(state):
            return state

        return lax.cond(first <= last_row, compute, skipped, inner)

    weighted, total = lax.fori_loop(0, count, one_block, init)
    result = weighted / total[..., None]
    attended = (
        jnp.transpose(result, (2, 0, 1, 3)).reshape(tok_dev, gate_heads * HEAD).astype(jnp.bfloat16)
    )
    out_ret, out_att = (
        lax.all_gather(w_out_ret, "sp", axis=1, tiled=True),
        lax.all_gather(w_out_att, "sp", axis=1, tiled=True),
    )
    return lax.psum_scatter(
        (
            jnp.dot(retained, out_ret, preferred_element_type=jnp.float32)
            + jnp.dot(attended, out_att, preferred_element_type=jnp.float32)
        ).astype(jnp.bfloat16),
        "tp",
        scatter_dimension=0,
        tiled=True,
    )


def choose(n, m, *arrays):
    tokens, w_key_ret, w_out_ret = arrays[0], arrays[3], arrays[8]
    whole_tiles = w_out_ret.shape[1] % LANES == 0 and w_key_ret.shape[0] % LANES == 0
    if whole_tiles and tokens.shape[0] * m == SPAN and arrays[7].shape[1] == HEAD:
        return body(n, m, *arrays)
    return plain_body(*arrays)


def solution(mesh):
    return jax.shard_map(
        functools.partial(choose, mesh.shape["sp"], mesh.shape["tp"]),
        mesh=mesh,
        in_specs=(
            P(("sp", "tp"), None),
            P(),
            P("sp", "tp"),
            P("sp", "tp"),
            P("sp", "tp"),
            P("sp", "tp"),
            P("sp", "tp"),
            P("sp", "tp"),
            P("tp", "sp"),
            P("tp", "sp"),
            P("sp", "tp"),
            P("tp", None),
        ),
        out_specs=P(("sp", "tp"), None),
        check_vma=False,
    )
```

```python
import functools

import jax
import jax.numpy as jnp
import numpy as np
from jax import lax
from jax.experimental import pallas as pl
from jax.experimental.pallas import tpu as pltpu
from jax.sharding import PartitionSpec as P

HEAD = 64
EPS = 1e-06
THETA = 10000.0
F32 = jnp.float32
BF16 = jnp.bfloat16
MESH = pl.DeviceIdType.MESH
SPAN = 256
KEY_SPAN = 256
LANES = 128
CHUNKS = (4, 4, 4, 2)
HIGH = lax.Precision.HIGHEST


def ring_to_sp(place, n):
    if n % 2:
        return place
    back = place // (n // 2)
    return (1 - back) * 2 * place + back * (2 * (n - 1 - place) + 1)


def sp_to_ring(index, n):
    if n % 2:
        return index
    odd, pair = index % 2, index // 2
    return (1 - odd) * pair + odd * (n - 1 - pair)


def dot(a, b, dims=((1,), (0,))):
    return lax.dot_general(a, b, (dims, ((), ())), preferred_element_type=F32)


def kernel(
    n,
    m,
    heads,
    chunks,
    tok_hbm,
    gain_ref,
    wq_ret_hbm,
    wk_ret_hbm,
    wv_ret_hbm,
    wq_att_hbm,
    wk_att_hbm,
    wv_att_hbm,
    wo_ret_hbm,
    wo_att_hbm,
    table_hbm,
    logs_ref,
    gate_ref,
    out_ref,
    tokens,
    wq_ret,
    wk_ret,
    wv_ret,
    wq_att,
    wk_att,
    wv_att,
    table,
    xbuf,
    abuf,
    bbuf,
    obuf,
    kvbuf,
    state,
    num,
    den,
    outbuf,
    rsbuf,
    *sems,
):
    (load, x_send, x_recv, a_send, a_recv, b_send, b_recv, o_send, o_recv, k_send, k_recv, r_send,
     r_recv) = sems
    me = lax.axis_index("sp")
    mine = lax.axis_index("tp")
    place = sp_to_ring(me, n)
    right = ring_to_sp((place + 1) % n, n)
    left = ring_to_sp((place + n - 1) % n, n)
    tok = xbuf.shape[0]
    rows = tok // m
    width = heads * HEAD

    half_o = wo_ret_hbm.shape[0]
    loads = [
        pltpu.make_async_copy(source, target, load.at[k])
        for k, (source, target) in enumerate((
            (wk_att_hbm, wk_att),
            (wv_att_hbm, wv_att),
            (wk_ret_hbm, wk_ret),
            (wv_ret_hbm, wv_ret),
            (tok_hbm, tokens),
            (wq_att_hbm, wq_att),
            (wq_ret_hbm, wq_ret),
            (table_hbm.at[pl.ds(pl.multiple_of(me * tok, tok), tok)], table),
            (wo_ret_hbm, obuf.at[me, pl.ds(0, half_o)]),
            (wo_att_hbm, obuf.at[me, pl.ds(half_o, wo_att_hbm.shape[0])]),
        ))
    ]
    for copy in loads:
        copy.start()

    barrier = pltpu.get_barrier_semaphore()
    for other in (left, right):
        pl.semaphore_signal(barrier, inc=1, device_id={"sp": other}, device_id_type=MESH)
    for r in range(1, m):
        pl.semaphore_signal(barrier, inc=1, device_id={"tp": (mine + r) % m}, device_id_type=MESH)

    for copy in loads[:4]:
        copy.wait()
    abuf[me, :, :HEAD] = wk_att[...]
    abuf[me, :, HEAD : 2 * HEAD] = wv_att[...]
    abuf[me, :, 2 * HEAD : 2 * HEAD + width] = wk_ret[...]
    abuf[me, :, 2 * HEAD + width :] = wv_ret[...]
    pl.semaphore_wait(barrier, 2 + m - 1)

    def ring_copy(buf, send, recv, pieces, step, way, chunk, arriving):
        hops = step + 1 if arriving else step
        owner = ring_to_sp((place + (n - hops if way == 0 else hops)) % n, n)
        half = buf.shape[1] // 2
        piece = half // pieces
        span = pl.ds(way * half + chunk * piece, piece)
        return pltpu.make_async_remote_copy(
            src_ref=buf.at[owner, span],
            dst_ref=buf.at[owner, span],
            send_sem=send.at[way, step, chunk],
            recv_sem=recv.at[way, step, chunk],
            device_id={"sp": right if way == 0 else left},
            device_id_type=MESH,
        )

    started = []

    def ring_step(group, step):
        for chunk in range(group[3]):
            for way in range(2):
                if step > 0:
                    ring_copy(*group, step - 1, way, chunk, True).wait_recv()
                if step < n - 1:
                    copy = ring_copy(*group, step, way, chunk, False)
                    copy.start()
                    started.append(copy)

    ring_a = (abuf, a_send, a_recv, chunks[0])
    ring_b = (bbuf, b_send, b_recv, chunks[1])
    ring_o = (obuf, o_send, o_recv, chunks[2])
    ring_k = (kvbuf, k_send, k_recv, chunks[3])

    ring_step(ring_a, 0)
    loads[4].wait()
    values = tokens[...].astype(F32)
    scale = lax.rsqrt(jnp.mean(values * values, axis=-1, keepdims=True) + EPS)
    own = pl.ds(mine * rows, rows)
    xbuf[own, :] = (values * scale * gain_ref[...]).astype(BF16)
    for r in range(1, m):
        copy = pltpu.make_async_remote_copy(
            src_ref=xbuf.at[own],
            dst_ref=xbuf.at[own],
            send_sem=x_send.at[r - 1],
            recv_sem=x_recv.at[r - 1],
            device_id={"tp": (mine + r) % m},
            device_id_type=MESH,
        )
        copy.start()
        started.append(copy)
    ring_step(ring_a, 1)
    for copy in loads[5:]:
        copy.wait()
    bbuf[me, :, :width] = wq_att[...]
    bbuf[me, :, width:] = wq_ret[...]
    ring_step(ring_a, 2)

    lines = lax.broadcasted_iota(jnp.int32, (tok, tok), 0)
    across = lax.broadcasted_iota(jnp.int32, (tok, tok), 1)
    causal = lines >= across
    upto = jnp.where(lines <= across, 1.0, 0.0)
    logs = jnp.concatenate([logs_ref[...], jnp.zeros((8 - heads, tok), F32)], axis=0)
    turned = lax.dot_general(
        logs, upto, (((1,), (0,)), ((), ())),
        preferred_element_type=F32, precision=lax.Precision.HIGHEST,
    )
    fill = jnp.zeros((LANES - 8, tok), F32)
    within = jnp.concatenate([turned, fill], axis=0).T
    gates_own = gate_ref[:, pl.ds(pl.multiple_of(me * tok, tok), tok)]
    gate_col = jnp.concatenate(
        [gates_own, jnp.zeros((LANES - heads, tok), F32)], axis=0
    ).T
    cosine, sine = table[:, : HEAD // 2], table[:, HEAD // 2 :]

    for step in range(3, n - 1):
        ring_step(ring_a, step)
    ring_step(ring_b, 0)
    for r in range(1, m):
        other = pl.ds(((mine + m - r) % m) * rows, rows)
        pltpu.make_async_remote_copy(
            src_ref=xbuf.at[other],
            dst_ref=xbuf.at[other],
            send_sem=x_send.at[r - 1],
            recv_sem=x_recv.at[r - 1],
            device_id={"tp": (mine + r) % m},
            device_id_type=MESH,
        ).wait_recv()
    ring_step(ring_a, n - 1)
    ring_step(ring_b, 1)

    def rope(field):
        half = HEAD // 2
        first, second = field[:, :half], field[:, half:]
        return jnp.concatenate(
            [first * cosine - second * sine, first * sine + second * cosine], axis=-1
        )

    proj = dot(xbuf[...], abuf[...].reshape(-1, abuf.shape[2]))
    pair = proj[:, : 2 * HEAD].astype(BF16)
    keys, vals, updates, marks = [], [], [], []
    for h in range(heads):
        base = 2 * HEAD + h * HEAD
        key = rope(proj[:, base : base + HEAD]).astype(BF16)
        val = proj[:, base + width : base + width + HEAD].astype(BF16)
        column = within[:, h : h + 1]
        last = column[tok - 1 :, :]
        faded = (key.astype(F32) * jnp.exp(last - column)).astype(BF16)
        updates.append(dot(faded, val, ((0,), (0,))))
        high = last.astype(BF16).astype(F32)
        low = last - high
        marks.append(jnp.broadcast_to(high, (8, HEAD)))
        marks.append(jnp.broadcast_to(low, (8, HEAD)))
        keys.append(key)
        vals.append(val)
    kvbuf[me, :tok, :] = pair
    marks.append(jnp.zeros((HEAD - 16 * heads, HEAD), F32))
    blocks = updates + [jnp.concatenate(marks, axis=0)]
    if len(blocks) % 2:
        blocks.append(jnp.zeros((HEAD, HEAD), F32))
    for k in range(0, len(blocks), 2):
        both = jnp.concatenate(blocks[k : k + 2], axis=1).astype(BF16)
        kvbuf[me, tok + k // 2 * HEAD : tok + (k // 2 + 1) * HEAD, :] = both

    def piece_of(index, k):
        lanes = slice(k % 2 * HEAD, (k % 2 + 1) * HEAD)
        return kvbuf[index, tok + k // 2 * HEAD : tok + (k // 2 + 1) * HEAD, lanes].astype(F32)

    for step in range(n - 1):
        ring_step(ring_k, step)
        if step == n - 2:
            ring_step(ring_o, 0)
        if step + 2 <= n - 1:
            ring_step(ring_b, step + 2)

    projq = dot(xbuf[...], bbuf[...].reshape(-1, bbuf.shape[2]))
    ring_step(ring_o, 1)
    local, lifts = [], []
    for h in range(heads):
        base = width + h * HEAD
        query = (rope(projq[:, base : base + HEAD]) * HEAD ** (-0.5)).astype(BF16)
        column = within[:, h : h + 1]
        gap = jnp.where(causal, column - turned[h : h + 1, :], 0.0)
        scores = dot(query, keys[h], ((1,), (1,)))
        weights = jnp.where(causal, scores * jnp.exp(gap), 0.0).astype(BF16)
        local.append(dot(weights, vals[h]))
        lifts.append((query.astype(F32) * jnp.exp(column)).astype(BF16))
    ring_step(ring_o, 2)

    queries = [
        (projq[:, h * HEAD : (h + 1) * HEAD] * HEAD ** (-0.5)).astype(BF16) for h in range(heads)
    ]

    def attend(index, masked):
        block = kvbuf[index, :tok, :]
        key, val = block[:, :HEAD], block[:, HEAD:]
        gates = gate_ref[:, pl.ds(pl.multiple_of(index * tok, tok), tok)]
        for h in range(heads):
            logits = dot(queries[h], key, ((1,), (1,)))
            logits = logits + gate_col[:, h : h + 1] - gates[h : h + 1, :]
            if masked:
                logits = jnp.where(causal, logits, -jnp.inf)
            weights = jnp.exp(logits)
            den[h] += jnp.broadcast_to(jnp.sum(weights, axis=-1, keepdims=True), (tok, HEAD))
            num[h] += dot(weights.astype(BF16), val)

    den[...] = jnp.zeros_like(den)
    num[...] = jnp.zeros_like(num)
    state[...] = jnp.zeros_like(state)
    attend(me, True)
    ring_step(ring_k, n - 1)
    for j in range(n - 1):
        def earlier(j=j):
            marked = piece_of(j, heads)
            for h in range(heads):
                total = marked[16 * h : 16 * h + 1] + marked[16 * h + 8 : 16 * h + 9]
                state[h] = jnp.exp(total) * state[h] + piece_of(j, h)
            attend(j, False)

        pl.when(me > j)(earlier)
        if 3 + j <= n - 1:
            ring_step(ring_o, 3 + j)
    for step in range(3 + n - 1, n):
        ring_step(ring_o, step)

    retained, attended = [], []
    for h in range(heads):
        raw = local[h] + dot(lifts[h], state[h].astype(BF16))
        centre = jnp.mean(raw, axis=-1, keepdims=True)
        spread = jnp.mean(jnp.square(raw - centre), axis=-1, keepdims=True)
        retained.append(((raw - centre) * lax.rsqrt(spread + EPS)).astype(BF16))
        attended.append((num[h] / den[h]).astype(BF16))
    mixed = jnp.concatenate(retained + attended, axis=-1)

    def out_copy(r, part, span):
        return pltpu.make_async_remote_copy(
            src_ref=outbuf.at[(mine + r) % m, :, span],
            dst_ref=rsbuf.at[mine, :, span],
            send_sem=r_send.at[r - 1, part],
            recv_sem=r_recv.at[r - 1, part],
            device_id={"tp": (mine + r) % m},
            device_id_type=MESH,
        )

    columns = obuf.shape[2]
    group = 2 if n % 2 == 0 else 1
    for part in range(n // group):
        for k in range(part * group, part * group + group):
            share = dot(mixed, obuf[k]).astype(BF16)
            outbuf[:, :, k * columns : (k + 1) * columns] = share.reshape(m, rows, columns)
        span = pl.ds(part * group * columns, group * columns)
        for r in range(1, m):
            copy = out_copy(r, part, span)
            copy.start()
            started.append(copy)
    for part in range(n // group):
        span = pl.ds(part * group * columns, group * columns)
        total = outbuf[mine, :, span].astype(F32)
        for r in range(1, m):
            other = (mine + m - r) % m
            pltpu.make_async_remote_copy(
                src_ref=rsbuf.at[other, :, span],
                dst_ref=rsbuf.at[other, :, span],
                send_sem=r_send.at[r - 1, part],
                recv_sem=r_recv.at[r - 1, part],
                device_id={"tp": (mine + r) % m},
                device_id_type=MESH,
            ).wait_recv()
            total = total + rsbuf[other, :, span].astype(F32)
        out_ref[:, span] = total.astype(BF16)

    for copy in started:
        copy.wait_send()


def body(
    n,
    m,
    tokens,
    pre_gain,
    w_query_ret,
    w_key_ret,
    w_value_ret,
    w_query_att,
    w_key_att,
    w_value_att,
    w_out_ret,
    w_out_att,
    retain_log,
    forget_total,
):
    rows, depth = tokens.shape
    tok = rows * m
    heads = retain_log.shape[1]
    half = HEAD // 2
    inverse = np.float32(THETA) ** (-np.arange(half, dtype=np.float32) / np.float32(half))
    angles = np.arange(n * tok, dtype=np.float32)[:, None] * inverse[None, :]
    table = np.concatenate([np.cos(angles), np.sin(angles)], axis=1).astype(np.float32)
    chunks = CHUNKS
    wide_a = 2 * HEAD + 2 * heads * HEAD
    wide_b = 2 * heads * HEAD
    deep = w_key_ret.shape[0]
    deep_o = w_out_ret.shape[0] + w_out_att.shape[0]
    tall = tok + (heads // 2 + 1) * HEAD
    hbm = pl.BlockSpec(memory_space=pl.ANY)
    vmem = pl.BlockSpec(memory_space=pltpu.VMEM)
    dma = pltpu.SemaphoreType.DMA
    rings = [dma((2, n - 1, c)) for c in chunks for _ in range(2)]
    parts = n // 2 if n % 2 == 0 else n
    return pl.pallas_call(
        functools.partial(kernel, n, m, heads, chunks),
        out_shape=jax.ShapeDtypeStruct((rows, depth), BF16),
        in_specs=[hbm, vmem] + [hbm] * 9 + [vmem] * 2,
        out_specs=vmem,
        scratch_shapes=[
            pltpu.VMEM(tokens.shape, BF16),
            pltpu.VMEM(w_query_ret.shape, BF16),
            pltpu.VMEM(w_key_ret.shape, BF16),
            pltpu.VMEM(w_value_ret.shape, BF16),
            pltpu.VMEM(w_query_att.shape, BF16),
            pltpu.VMEM(w_key_att.shape, BF16),
            pltpu.VMEM(w_value_att.shape, BF16),
            pltpu.VMEM((tok, HEAD), F32),
            pltpu.VMEM((tok, depth), BF16),
            pltpu.VMEM((n, deep, wide_a), BF16),
            pltpu.VMEM((n, deep, wide_b), BF16),
            pltpu.VMEM((n, deep_o, w_out_ret.shape[1]), BF16),
            pltpu.VMEM((n, tall, 2 * HEAD), BF16),
            pltpu.VMEM((heads, HEAD, HEAD), F32),
            pltpu.VMEM((heads, tok, HEAD), F32),
            pltpu.VMEM((heads, tok, HEAD), F32),
            pltpu.VMEM((m, rows, depth), BF16),
            pltpu.VMEM((m, rows, depth), BF16),
            dma((10,)),
            dma((m - 1,)),
            dma((m - 1,)),
            *rings,
            dma((m - 1, parts)),
            dma((m - 1, parts)),
        ],
        compiler_params=pltpu.CompilerParams(
            collective_id=0, has_side_effects=True, vmem_limit_bytes=60 * 1024 * 1024
        ),
    )(
        tokens,
        pre_gain[None, :],
        w_query_ret,
        w_key_ret,
        w_value_ret,
        w_query_att,
        w_key_att,
        w_value_att,
        w_out_ret,
        w_out_att,
        jnp.asarray(table),
        retain_log.T,
        forget_total,
    )


def rotate(field, positions):
    half = field.shape[-1] // 2
    inverse = THETA ** (-jnp.arange(half, dtype=jnp.float32) / half)
    angles = positions[:, None] * inverse[None, :]
    cosine = jnp.cos(angles)[:, None, :]
    sine = jnp.sin(angles)[:, None, :]
    first_half = field[..., :half]
    second_half = field[..., half:]
    return jnp.concatenate(
        [first_half * cosine - second_half * sine, first_half * sine + second_half * cosine],
        axis=-1,
    )


def head_norm(values):
    centre = jnp.mean(values, axis=-1, keepdims=True)
    spread = jnp.mean(jnp.square(values - centre), axis=-1, keepdims=True)
    return (values - centre) * lax.rsqrt(spread + EPS)


def advance(state, pair):
    decay, update = pair
    return (jnp.exp(decay)[:, None, None] * state + update, state)


def plain_body(
    tokens,
    pre_gain,
    w_query_ret,
    w_key_ret,
    w_value_ret,
    w_query_att,
    w_key_att,
    w_value_att,
    w_out_ret,
    w_out_att,
    retain_log,
    forget_total,
):
    rows = tokens.astype(jnp.float32)
    normed = (
        rows * lax.rsqrt(jnp.mean(rows * rows, axis=-1, keepdims=True) + EPS) * pre_gain
    ).astype(jnp.bfloat16)
    gathered = lax.all_gather(normed, "tp", axis=0, tiled=True)
    tok_dev = gathered.shape[0]
    offset = lax.axis_index("sp") * tok_dev
    query_places = offset + jnp.arange(tok_dev, dtype=jnp.int32)
    positions = query_places.astype(jnp.float32)

    def blocked(values):
        return values.reshape((tok_dev // SPAN, SPAN) + values.shape[1:])

    pieces = (
        lax.all_gather(w_query_ret, "sp", axis=0, tiled=True),
        lax.all_gather(w_key_ret, "sp", axis=0, tiled=True),
        lax.all_gather(w_value_ret, "sp", axis=0, tiled=True),
        lax.all_gather(w_query_att, "sp", axis=0, tiled=True),
        lax.all_gather(w_key_att, "sp", axis=0, tiled=True),
        lax.all_gather(w_value_att, "sp", axis=0, tiled=True),
    )
    projected = tuple(
        (jnp.dot(gathered, piece, preferred_element_type=jnp.float32) for piece in pieces)
    )
    heads = retain_log.shape[1]
    shape = (tok_dev, heads, HEAD)
    query = blocked(
        (rotate(projected[0].reshape(shape), positions) * HEAD ** (-0.5)).astype(jnp.bfloat16)
    )
    key_rows = blocked(rotate(projected[1].reshape(shape), positions).astype(jnp.bfloat16))
    value_rows = blocked(projected[2].astype(jnp.bfloat16).reshape(shape))
    within = jnp.cumsum(blocked(retain_log), axis=1)
    causal = jnp.arange(SPAN)[:, None] >= jnp.arange(SPAN)[None, :]
    scores = jnp.einsum("bthd,bshd->bhts", query, key_rows, preferred_element_type=jnp.float32)
    turned = jnp.transpose(within, (0, 2, 1))
    gap = jnp.where(causal, turned[:, :, :, None] - turned[:, :, None, :], 0.0)
    weights = jnp.where(causal, scores * jnp.exp(gap), 0.0).astype(jnp.bfloat16)
    local = jnp.einsum("bhts,bshd->bthd", weights, value_rows, preferred_element_type=jnp.float32)
    last = within[:, -1]
    faded = (key_rows.astype(jnp.float32) * jnp.exp(last[:, None, :] - within)[..., None]).astype(
        jnp.bfloat16
    )
    updates = jnp.einsum("bshd,bshe->bhde", faded, value_rows, preferred_element_type=jnp.float32)
    zero_state = jnp.zeros((heads, HEAD, HEAD), jnp.float32)
    final, _ = lax.scan(advance, zero_state, (last, updates))
    decay_total = jnp.sum(last, axis=0)
    own_state = final.reshape(heads, HEAD * HEAD)
    every_total = lax.all_gather(
        decay_total[None].astype(jnp.bfloat16), "sp", axis=0, tiled=True
    ).astype(jnp.float32)
    every_state = lax.all_gather(
        own_state[None].astype(jnp.bfloat16), "sp", axis=0, tiled=True
    ).astype(jnp.float32)
    device_order = jnp.arange(every_total.shape[0], dtype=jnp.int32)[:, None]
    earlier = device_order < lax.axis_index("sp")
    before = jnp.sum(jnp.where(earlier, every_total, 0.0), axis=0)
    through = jnp.cumsum(every_total, axis=0)
    fading = jnp.where(earlier, jnp.exp(jnp.where(earlier, before[None, :] - through, 0.0)), 0.0)
    incoming = jnp.einsum("jh,jhe->he", fading, every_state, precision=HIGH)
    _, befores = lax.scan(advance, incoming.reshape(heads, HEAD, HEAD), (last, updates))
    lifted = (query.astype(jnp.float32) * jnp.exp(within)[..., None]).astype(jnp.bfloat16)
    carried = jnp.einsum(
        "bthd,bhde->bthe", lifted, befores.astype(jnp.bfloat16), preferred_element_type=jnp.float32
    )
    retained = (
        head_norm((local + carried).reshape(shape))
        .astype(jnp.bfloat16)
        .reshape(tok_dev, heads * HEAD)
    )
    raw_key = projected[4]
    gate_heads = forget_total.shape[0]
    kv_local = raw_key.shape[1] // HEAD
    group = gate_heads // kv_local
    query = (
        (projected[3] * HEAD ** (-0.5)).astype(jnp.bfloat16).reshape(tok_dev, kv_local, group, HEAD)
    )
    key_rows = raw_key.astype(jnp.bfloat16)
    value_rows = projected[5].astype(jnp.bfloat16)
    gate_rows = lax.dynamic_slice_in_dim(forget_total, offset, tok_dev, 1).reshape(
        kv_local, group, tok_dev
    )
    last_row = offset + tok_dev - 1
    init = (
        jnp.zeros((kv_local, group, tok_dev, HEAD), jnp.float32),
        jnp.zeros((kv_local, group, tok_dev), jnp.float32),
    )
    key_piece = lax.all_gather(key_rows, "sp", axis=0, tiled=True)
    value_piece = lax.all_gather(value_rows, "sp", axis=0, tiled=True)
    count = key_piece.shape[0] // KEY_SPAN

    def one_block(index, inner):
        first = index * KEY_SPAN

        def compute(state):
            weighted, total = state
            key_block = lax.dynamic_slice_in_dim(key_piece, index * KEY_SPAN, KEY_SPAN, 0).reshape(
                KEY_SPAN, kv_local, HEAD
            )
            value_block = lax.dynamic_slice_in_dim(
                value_piece, index * KEY_SPAN, KEY_SPAN, 0
            ).reshape(KEY_SPAN, kv_local, HEAD)
            gate_keys = lax.dynamic_slice_in_dim(forget_total, first, KEY_SPAN, 1).reshape(
                kv_local, group, KEY_SPAN
            )
            scores = jnp.einsum(
                "tcgd,scd->cgts", query, key_block, preferred_element_type=jnp.float32
            )
            logits = scores + gate_rows[:, :, :, None] - gate_keys[:, :, None, :]
            allowed = (first + jnp.arange(KEY_SPAN, dtype=jnp.int32))[None, :] <= query_places[
                :, None
            ]
            weights = jnp.exp(jnp.where(allowed, logits, -jnp.inf))
            total = total + jnp.sum(weights, axis=-1)
            weighted = weighted + jnp.einsum(
                "cgts,scd->cgtd",
                weights.astype(jnp.bfloat16),
                value_block,
                preferred_element_type=jnp.float32,
            )
            return (weighted, total)

        def skipped(state):
            return state

        return lax.cond(first <= last_row, compute, skipped, inner)

    weighted, total = lax.fori_loop(0, count, one_block, init)
    result = weighted / total[..., None]
    attended = (
        jnp.transpose(result, (2, 0, 1, 3)).reshape(tok_dev, gate_heads * HEAD).astype(jnp.bfloat16)
    )
    out_ret, out_att = (
        lax.all_gather(w_out_ret, "sp", axis=1, tiled=True),
        lax.all_gather(w_out_att, "sp", axis=1, tiled=True),
    )
    return lax.psum_scatter(
        (
            jnp.dot(retained, out_ret, preferred_element_type=jnp.float32)
            + jnp.dot(attended, out_att, preferred_element_type=jnp.float32)
        ).astype(jnp.bfloat16),
        "tp",
        scatter_dimension=0,
        tiled=True,
    )


def choose(n, m, *arrays):
    tokens, w_key_ret, w_out_ret = arrays[0], arrays[3], arrays[8]
    whole_tiles = w_out_ret.shape[1] % LANES == 0 and w_key_ret.shape[0] % LANES == 0
    heads = arrays[10].shape[1]
    small = 16 * heads <= HEAD and arrays[7].shape[1] == HEAD and arrays[11].shape[0] == heads
    if whole_tiles and small and tokens.shape[0] * m == SPAN:
        return body(n, m, *arrays)
    return plain_body(*arrays)


def solution(mesh):
    return jax.shard_map(
        functools.partial(choose, mesh.shape["sp"], mesh.shape["tp"]),
        mesh=mesh,
        in_specs=(
            P(("sp", "tp"), None),
            P(),
            P("sp", "tp"),
            P("sp", "tp"),
            P("sp", "tp"),
            P("sp", "tp"),
            P("sp", "tp"),
            P("sp", "tp"),
            P("tp", "sp"),
            P("tp", "sp"),
            P("sp", "tp"),
            P("tp", None),
        ),
        out_specs=P(("sp", "tp"), None),
        check_vma=False,
    )
```

```python
import functools

import jax
import jax.numpy as jnp
import numpy as np
from jax import lax
from jax.experimental import pallas as pl
from jax.experimental.pallas import tpu as pltpu
from jax.sharding import PartitionSpec as P

HEAD = 64
EPS = 1e-06
THETA = 10000.0
F32 = jnp.float32
BF16 = jnp.bfloat16
MESH = pl.DeviceIdType.MESH
SPAN = 256
KEY_SPAN = 256
LANES = 128
CHUNKS = (4, 4, 4, 2)
HIGH = lax.Precision.HIGHEST


def ring_to_sp(place, n):
    if n % 2:
        return place
    back = place // (n // 2)
    return (1 - back) * 2 * place + back * (2 * (n - 1 - place) + 1)


def sp_to_ring(index, n):
    if n % 2:
        return index
    odd, pair = index % 2, index // 2
    return (1 - odd) * pair + odd * (n - 1 - pair)


def dot(a, b, dims=((1,), (0,))):
    return lax.dot_general(a, b, (dims, ((), ())), preferred_element_type=F32)


def kernel(
    n,
    m,
    heads,
    chunks,
    tok_hbm,
    gain_ref,
    wq_ret_hbm,
    wk_ret_hbm,
    wv_ret_hbm,
    wq_att_hbm,
    wk_att_hbm,
    wv_att_hbm,
    wo_ret_hbm,
    wo_att_hbm,
    table_hbm,
    logs_ref,
    gate_ref,
    out_ref,
    tokens,
    table,
    xbuf,
    abuf,
    bbuf,
    obuf,
    kvbuf,
    state,
    num,
    den,
    outbuf,
    rsbuf,
    *sems,
):
    (load, x_send, x_recv, a_send, a_recv, b_send, b_recv, o_send, o_recv, k_send, k_recv, r_send,
     r_recv) = sems
    me = lax.axis_index("sp")
    mine = lax.axis_index("tp")
    place = sp_to_ring(me, n)
    right = ring_to_sp((place + 1) % n, n)
    left = ring_to_sp((place + n - 1) % n, n)
    tok = xbuf.shape[0]
    rows = tok // m
    width = heads * HEAD

    half_o = wo_ret_hbm.shape[0]
    loads = [
        pltpu.make_async_copy(source, target, load.at[k])
        for k, (source, target) in enumerate((
            (wk_att_hbm, abuf.at[me, pl.ds(0, HEAD)]),
            (wv_att_hbm, abuf.at[me, pl.ds(HEAD, HEAD)]),
            (wk_ret_hbm, abuf.at[me, pl.ds(2 * HEAD, width)]),
            (wv_ret_hbm, abuf.at[me, pl.ds(2 * HEAD + width, width)]),
            (tok_hbm, tokens),
            (wq_att_hbm, bbuf.at[me, pl.ds(0, width)]),
            (wq_ret_hbm, bbuf.at[me, pl.ds(width, width)]),
            (table_hbm.at[pl.ds(pl.multiple_of(me * tok, tok), tok)], table),
            (wo_ret_hbm, obuf.at[me, pl.ds(0, half_o)]),
            (wo_att_hbm, obuf.at[me, pl.ds(half_o, wo_att_hbm.shape[0])]),
        ))
    ]
    for copy in loads:
        copy.start()

    barrier = pltpu.get_barrier_semaphore()
    for other in (left, right):
        pl.semaphore_signal(barrier, inc=1, device_id={"sp": other}, device_id_type=MESH)
    for r in range(1, m):
        pl.semaphore_signal(barrier, inc=1, device_id={"tp": (mine + r) % m}, device_id_type=MESH)

    for copy in loads[:4]:
        copy.wait()
    pl.semaphore_wait(barrier, 2 + m - 1)

    def ring_copy(buf, send, recv, pieces, step, way, chunk, arriving):
        hops = step + 1 if arriving else step
        owner = ring_to_sp((place + (n - hops if way == 0 else hops)) % n, n)
        half = buf.shape[1] // 2
        piece = half // pieces
        span = pl.ds(way * half + chunk * piece, piece)
        return pltpu.make_async_remote_copy(
            src_ref=buf.at[owner, span],
            dst_ref=buf.at[owner, span],
            send_sem=send.at[way, step, chunk],
            recv_sem=recv.at[way, step, chunk],
            device_id={"sp": right if way == 0 else left},
            device_id_type=MESH,
        )

    started = []

    def ring_step(group, step):
        for chunk in range(group[3]):
            for way in range(2):
                if step > 0:
                    ring_copy(*group, step - 1, way, chunk, True).wait_recv()
                if step < n - 1:
                    copy = ring_copy(*group, step, way, chunk, False)
                    copy.start()
                    started.append(copy)

    ring_a = (abuf, a_send, a_recv, chunks[0])
    ring_b = (bbuf, b_send, b_recv, chunks[1])
    ring_o = (obuf, o_send, o_recv, chunks[2])
    ring_k = (kvbuf, k_send, k_recv, chunks[3])

    ring_step(ring_a, 0)
    loads[4].wait()
    values = tokens[...].astype(F32)
    scale = lax.rsqrt(jnp.mean(values * values, axis=-1, keepdims=True) + EPS)
    own = pl.ds(mine * rows, rows)
    xbuf[own, :] = (values * scale * gain_ref[...]).astype(BF16)
    for r in range(1, m):
        copy = pltpu.make_async_remote_copy(
            src_ref=xbuf.at[own],
            dst_ref=xbuf.at[own],
            send_sem=x_send.at[r - 1],
            recv_sem=x_recv.at[r - 1],
            device_id={"tp": (mine + r) % m},
            device_id_type=MESH,
        )
        copy.start()
        started.append(copy)
    ring_step(ring_a, 1)
    for copy in loads[5:]:
        copy.wait()
    ring_step(ring_a, 2)

    lines = lax.broadcasted_iota(jnp.int32, (tok, tok), 0)
    across = lax.broadcasted_iota(jnp.int32, (tok, tok), 1)
    causal = lines >= across
    upto = jnp.where(lines <= across, 1.0, 0.0)
    logs = jnp.concatenate([logs_ref[...], jnp.zeros((8 - heads, tok), F32)], axis=0)
    turned = lax.dot_general(
        logs, upto, (((1,), (0,)), ((), ())),
        preferred_element_type=F32, precision=lax.Precision.HIGHEST,
    )
    fill = jnp.zeros((LANES - 8, tok), F32)
    within = jnp.concatenate([turned, fill], axis=0).T
    gates_own = gate_ref[:, pl.ds(pl.multiple_of(me * tok, tok), tok)]
    gate_col = jnp.concatenate(
        [gates_own, jnp.zeros((LANES - heads, tok), F32)], axis=0
    ).T
    cosine, sine = table[:, : HEAD // 2], table[:, HEAD // 2 :]

    for step in range(3, n - 1):
        ring_step(ring_a, step)
    ring_step(ring_b, 0)
    for r in range(1, m):
        other = pl.ds(((mine + m - r) % m) * rows, rows)
        pltpu.make_async_remote_copy(
            src_ref=xbuf.at[other],
            dst_ref=xbuf.at[other],
            send_sem=x_send.at[r - 1],
            recv_sem=x_recv.at[r - 1],
            device_id={"tp": (mine + r) % m},
            device_id_type=MESH,
        ).wait_recv()
    ring_step(ring_a, n - 1)
    ring_step(ring_b, 1)

    def rope(field):
        half = HEAD // 2
        first, second = field[:, :half], field[:, half:]
        return jnp.concatenate(
            [first * cosine - second * sine, first * sine + second * cosine], axis=-1
        )

    def project(buf):
        deep = buf.shape[2]
        return sum(
            dot(xbuf[:, k * deep : (k + 1) * deep], buf[k], ((1,), (1,))) for k in range(n)
        )

    proj = project(abuf)
    pair = proj[:, : 2 * HEAD].astype(BF16)
    keys, vals, updates, marks = [], [], [], []
    for h in range(heads):
        base = 2 * HEAD + h * HEAD
        key = rope(proj[:, base : base + HEAD]).astype(BF16)
        val = proj[:, base + width : base + width + HEAD].astype(BF16)
        column = within[:, h : h + 1]
        last = column[tok - 1 :, :]
        faded = (key.astype(F32) * jnp.exp(last - column)).astype(BF16)
        updates.append(dot(faded, val, ((0,), (0,))))
        high = last.astype(BF16).astype(F32)
        low = last - high
        marks.append(jnp.broadcast_to(high, (8, HEAD)))
        marks.append(jnp.broadcast_to(low, (8, HEAD)))
        keys.append(key)
        vals.append(val)
    kvbuf[me, :tok, :] = pair
    marks.append(jnp.zeros((HEAD - 16 * heads, HEAD), F32))
    blocks = updates + [jnp.concatenate(marks, axis=0)]
    if len(blocks) % 2:
        blocks.append(jnp.zeros((HEAD, HEAD), F32))
    for k in range(0, len(blocks), 2):
        both = jnp.concatenate(blocks[k : k + 2], axis=1).astype(BF16)
        kvbuf[me, tok + k // 2 * HEAD : tok + (k // 2 + 1) * HEAD, :] = both

    def piece_of(index, k):
        lanes = slice(k % 2 * HEAD, (k % 2 + 1) * HEAD)
        return kvbuf[index, tok + k // 2 * HEAD : tok + (k // 2 + 1) * HEAD, lanes].astype(F32)

    for step in range(n - 1):
        ring_step(ring_k, step)
        if step == n - 2:
            ring_step(ring_o, 0)
        if step + 2 <= n - 1:
            ring_step(ring_b, step + 2)

    projq = project(bbuf)
    ring_step(ring_o, 1)
    local, lifts = [], []
    for h in range(heads):
        base = width + h * HEAD
        query = (rope(projq[:, base : base + HEAD]) * HEAD ** (-0.5)).astype(BF16)
        column = within[:, h : h + 1]
        gap = jnp.where(causal, column - turned[h : h + 1, :], 0.0)
        scores = dot(query, keys[h], ((1,), (1,)))
        weights = jnp.where(causal, scores * jnp.exp(gap), 0.0).astype(BF16)
        local.append(dot(weights, vals[h]))
        lifts.append((query.astype(F32) * jnp.exp(column)).astype(BF16))
    ring_step(ring_o, 2)

    queries = [
        (projq[:, h * HEAD : (h + 1) * HEAD] * HEAD ** (-0.5)).astype(BF16) for h in range(heads)
    ]

    def attend(index, masked):
        block = kvbuf[index, :tok, :]
        key, val = block[:, :HEAD], block[:, HEAD:]
        gates = gate_ref[:, pl.ds(pl.multiple_of(index * tok, tok), tok)]
        for h in range(heads):
            logits = dot(queries[h], key, ((1,), (1,)))
            logits = logits + gate_col[:, h : h + 1] - gates[h : h + 1, :]
            if masked:
                logits = jnp.where(causal, logits, -jnp.inf)
            weights = jnp.exp(logits)
            den[h] += jnp.broadcast_to(jnp.sum(weights, axis=-1, keepdims=True), (tok, HEAD))
            num[h] += dot(weights.astype(BF16), val)

    den[...] = jnp.zeros_like(den)
    num[...] = jnp.zeros_like(num)
    state[...] = jnp.zeros_like(state)
    attend(me, True)
    ring_step(ring_k, n - 1)
    for j in range(n - 1):
        def earlier(j=j):
            marked = piece_of(j, heads)
            for h in range(heads):
                total = marked[16 * h : 16 * h + 1] + marked[16 * h + 8 : 16 * h + 9]
                state[h] = jnp.exp(total) * state[h] + piece_of(j, h)
            attend(j, False)

        pl.when(me > j)(earlier)
        if 3 + j <= n - 1:
            ring_step(ring_o, 3 + j)
    for step in range(3 + n - 1, n):
        ring_step(ring_o, step)

    retained, attended = [], []
    for h in range(heads):
        raw = local[h] + dot(lifts[h], state[h].astype(BF16))
        centre = jnp.mean(raw, axis=-1, keepdims=True)
        spread = jnp.mean(jnp.square(raw - centre), axis=-1, keepdims=True)
        retained.append(((raw - centre) * lax.rsqrt(spread + EPS)).astype(BF16))
        attended.append((num[h] / den[h]).astype(BF16))
    mixed = jnp.concatenate(retained + attended, axis=-1)

    def out_copy(r, part, span):
        return pltpu.make_async_remote_copy(
            src_ref=outbuf.at[(mine + r) % m, :, span],
            dst_ref=rsbuf.at[mine, :, span],
            send_sem=r_send.at[r - 1, part],
            recv_sem=r_recv.at[r - 1, part],
            device_id={"tp": (mine + r) % m},
            device_id_type=MESH,
        )

    columns = obuf.shape[2]
    group = 2 if n % 2 == 0 else 1
    for part in range(n // group):
        for k in range(part * group, part * group + group):
            share = dot(mixed, obuf[k]).astype(BF16)
            outbuf[:, :, k * columns : (k + 1) * columns] = share.reshape(m, rows, columns)
        span = pl.ds(part * group * columns, group * columns)
        for r in range(1, m):
            copy = out_copy(r, part, span)
            copy.start()
            started.append(copy)
    for part in range(n // group):
        span = pl.ds(part * group * columns, group * columns)
        total = outbuf[mine, :, span].astype(F32)
        for r in range(1, m):
            other = (mine + m - r) % m
            pltpu.make_async_remote_copy(
                src_ref=rsbuf.at[other, :, span],
                dst_ref=rsbuf.at[other, :, span],
                send_sem=r_send.at[r - 1, part],
                recv_sem=r_recv.at[r - 1, part],
                device_id={"tp": (mine + r) % m},
                device_id_type=MESH,
            ).wait_recv()
            total = total + rsbuf[other, :, span].astype(F32)
        out_ref[:, span] = total.astype(BF16)

    for copy in started:
        copy.wait_send()


def body(
    n,
    m,
    tokens,
    pre_gain,
    w_query_ret,
    w_key_ret,
    w_value_ret,
    w_query_att,
    w_key_att,
    w_value_att,
    w_out_ret,
    w_out_att,
    retain_log,
    forget_total,
):
    rows, depth = tokens.shape
    tok = rows * m
    heads = retain_log.shape[1]
    half = HEAD // 2
    inverse = np.float32(THETA) ** (-np.arange(half, dtype=np.float32) / np.float32(half))
    angles = np.arange(n * tok, dtype=np.float32)[:, None] * inverse[None, :]
    table = np.concatenate([np.cos(angles), np.sin(angles)], axis=1).astype(np.float32)
    chunks = CHUNKS
    wide_a = 2 * HEAD + 2 * heads * HEAD
    wide_b = 2 * heads * HEAD
    deep = w_key_ret.shape[0]
    deep_o = w_out_ret.shape[0] + w_out_att.shape[0]
    tall = tok + (heads // 2 + 1) * HEAD
    hbm = pl.BlockSpec(memory_space=pl.ANY)
    vmem = pl.BlockSpec(memory_space=pltpu.VMEM)
    dma = pltpu.SemaphoreType.DMA
    rings = [dma((2, n - 1, c)) for c in chunks for _ in range(2)]
    parts = n // 2 if n % 2 == 0 else n
    return pl.pallas_call(
        functools.partial(kernel, n, m, heads, chunks),
        out_shape=jax.ShapeDtypeStruct((rows, depth), BF16),
        in_specs=[hbm, vmem] + [hbm] * 9 + [vmem] * 2,
        out_specs=vmem,
        scratch_shapes=[
            pltpu.VMEM(tokens.shape, BF16),
            pltpu.VMEM((tok, HEAD), F32),
            pltpu.VMEM((tok, depth), BF16),
            pltpu.VMEM((n, wide_a, deep), BF16),
            pltpu.VMEM((n, wide_b, deep), BF16),
            pltpu.VMEM((n, deep_o, w_out_ret.shape[1]), BF16),
            pltpu.VMEM((n, tall, 2 * HEAD), BF16),
            pltpu.VMEM((heads, HEAD, HEAD), F32),
            pltpu.VMEM((heads, tok, HEAD), F32),
            pltpu.VMEM((heads, tok, HEAD), F32),
            pltpu.VMEM((m, rows, depth), BF16),
            pltpu.VMEM((m, rows, depth), BF16),
            dma((10,)),
            dma((m - 1,)),
            dma((m - 1,)),
            *rings,
            dma((m - 1, parts)),
            dma((m - 1, parts)),
        ],
        compiler_params=pltpu.CompilerParams(
            collective_id=0, has_side_effects=True, vmem_limit_bytes=60 * 1024 * 1024
        ),
    )(
        tokens,
        pre_gain[None, :],
        w_query_ret.T,
        w_key_ret.T,
        w_value_ret.T,
        w_query_att.T,
        w_key_att.T,
        w_value_att.T,
        w_out_ret,
        w_out_att,
        jnp.asarray(table),
        retain_log.T,
        forget_total,
    )


def rotate(field, positions):
    half = field.shape[-1] // 2
    inverse = THETA ** (-jnp.arange(half, dtype=jnp.float32) / half)
    angles = positions[:, None] * inverse[None, :]
    cosine = jnp.cos(angles)[:, None, :]
    sine = jnp.sin(angles)[:, None, :]
    first_half = field[..., :half]
    second_half = field[..., half:]
    return jnp.concatenate(
        [first_half * cosine - second_half * sine, first_half * sine + second_half * cosine],
        axis=-1,
    )


def head_norm(values):
    centre = jnp.mean(values, axis=-1, keepdims=True)
    spread = jnp.mean(jnp.square(values - centre), axis=-1, keepdims=True)
    return (values - centre) * lax.rsqrt(spread + EPS)


def advance(state, pair):
    decay, update = pair
    return (jnp.exp(decay)[:, None, None] * state + update, state)


def plain_body(
    tokens,
    pre_gain,
    w_query_ret,
    w_key_ret,
    w_value_ret,
    w_query_att,
    w_key_att,
    w_value_att,
    w_out_ret,
    w_out_att,
    retain_log,
    forget_total,
):
    rows = tokens.astype(jnp.float32)
    normed = (
        rows * lax.rsqrt(jnp.mean(rows * rows, axis=-1, keepdims=True) + EPS) * pre_gain
    ).astype(jnp.bfloat16)
    gathered = lax.all_gather(normed, "tp", axis=0, tiled=True)
    tok_dev = gathered.shape[0]
    offset = lax.axis_index("sp") * tok_dev
    query_places = offset + jnp.arange(tok_dev, dtype=jnp.int32)
    positions = query_places.astype(jnp.float32)

    def blocked(values):
        return values.reshape((tok_dev // SPAN, SPAN) + values.shape[1:])

    pieces = (
        lax.all_gather(w_query_ret, "sp", axis=0, tiled=True),
        lax.all_gather(w_key_ret, "sp", axis=0, tiled=True),
        lax.all_gather(w_value_ret, "sp", axis=0, tiled=True),
        lax.all_gather(w_query_att, "sp", axis=0, tiled=True),
        lax.all_gather(w_key_att, "sp", axis=0, tiled=True),
        lax.all_gather(w_value_att, "sp", axis=0, tiled=True),
    )
    projected = tuple(
        (jnp.dot(gathered, piece, preferred_element_type=jnp.float32) for piece in pieces)
    )
    heads = retain_log.shape[1]
    shape = (tok_dev, heads, HEAD)
    query = blocked(
        (rotate(projected[0].reshape(shape), positions) * HEAD ** (-0.5)).astype(jnp.bfloat16)
    )
    key_rows = blocked(rotate(projected[1].reshape(shape), positions).astype(jnp.bfloat16))
    value_rows = blocked(projected[2].astype(jnp.bfloat16).reshape(shape))
    within = jnp.cumsum(blocked(retain_log), axis=1)
    causal = jnp.arange(SPAN)[:, None] >= jnp.arange(SPAN)[None, :]
    scores = jnp.einsum("bthd,bshd->bhts", query, key_rows, preferred_element_type=jnp.float32)
    turned = jnp.transpose(within, (0, 2, 1))
    gap = jnp.where(causal, turned[:, :, :, None] - turned[:, :, None, :], 0.0)
    weights = jnp.where(causal, scores * jnp.exp(gap), 0.0).astype(jnp.bfloat16)
    local = jnp.einsum("bhts,bshd->bthd", weights, value_rows, preferred_element_type=jnp.float32)
    last = within[:, -1]
    faded = (key_rows.astype(jnp.float32) * jnp.exp(last[:, None, :] - within)[..., None]).astype(
        jnp.bfloat16
    )
    updates = jnp.einsum("bshd,bshe->bhde", faded, value_rows, preferred_element_type=jnp.float32)
    zero_state = jnp.zeros((heads, HEAD, HEAD), jnp.float32)
    final, _ = lax.scan(advance, zero_state, (last, updates))
    decay_total = jnp.sum(last, axis=0)
    own_state = final.reshape(heads, HEAD * HEAD)
    every_total = lax.all_gather(
        decay_total[None].astype(jnp.bfloat16), "sp", axis=0, tiled=True
    ).astype(jnp.float32)
    every_state = lax.all_gather(
        own_state[None].astype(jnp.bfloat16), "sp", axis=0, tiled=True
    ).astype(jnp.float32)
    device_order = jnp.arange(every_total.shape[0], dtype=jnp.int32)[:, None]
    earlier = device_order < lax.axis_index("sp")
    before = jnp.sum(jnp.where(earlier, every_total, 0.0), axis=0)
    through = jnp.cumsum(every_total, axis=0)
    fading = jnp.where(earlier, jnp.exp(jnp.where(earlier, before[None, :] - through, 0.0)), 0.0)
    incoming = jnp.einsum("jh,jhe->he", fading, every_state, precision=HIGH)
    _, befores = lax.scan(advance, incoming.reshape(heads, HEAD, HEAD), (last, updates))
    lifted = (query.astype(jnp.float32) * jnp.exp(within)[..., None]).astype(jnp.bfloat16)
    carried = jnp.einsum(
        "bthd,bhde->bthe", lifted, befores.astype(jnp.bfloat16), preferred_element_type=jnp.float32
    )
    retained = (
        head_norm((local + carried).reshape(shape))
        .astype(jnp.bfloat16)
        .reshape(tok_dev, heads * HEAD)
    )
    raw_key = projected[4]
    gate_heads = forget_total.shape[0]
    kv_local = raw_key.shape[1] // HEAD
    group = gate_heads // kv_local
    query = (
        (projected[3] * HEAD ** (-0.5)).astype(jnp.bfloat16).reshape(tok_dev, kv_local, group, HEAD)
    )
    key_rows = raw_key.astype(jnp.bfloat16)
    value_rows = projected[5].astype(jnp.bfloat16)
    gate_rows = lax.dynamic_slice_in_dim(forget_total, offset, tok_dev, 1).reshape(
        kv_local, group, tok_dev
    )
    last_row = offset + tok_dev - 1
    init = (
        jnp.zeros((kv_local, group, tok_dev, HEAD), jnp.float32),
        jnp.zeros((kv_local, group, tok_dev), jnp.float32),
    )
    key_piece = lax.all_gather(key_rows, "sp", axis=0, tiled=True)
    value_piece = lax.all_gather(value_rows, "sp", axis=0, tiled=True)
    count = key_piece.shape[0] // KEY_SPAN

    def one_block(index, inner):
        first = index * KEY_SPAN

        def compute(state):
            weighted, total = state
            key_block = lax.dynamic_slice_in_dim(key_piece, index * KEY_SPAN, KEY_SPAN, 0).reshape(
                KEY_SPAN, kv_local, HEAD
            )
            value_block = lax.dynamic_slice_in_dim(
                value_piece, index * KEY_SPAN, KEY_SPAN, 0
            ).reshape(KEY_SPAN, kv_local, HEAD)
            gate_keys = lax.dynamic_slice_in_dim(forget_total, first, KEY_SPAN, 1).reshape(
                kv_local, group, KEY_SPAN
            )
            scores = jnp.einsum(
                "tcgd,scd->cgts", query, key_block, preferred_element_type=jnp.float32
            )
            logits = scores + gate_rows[:, :, :, None] - gate_keys[:, :, None, :]
            allowed = (first + jnp.arange(KEY_SPAN, dtype=jnp.int32))[None, :] <= query_places[
                :, None
            ]
            weights = jnp.exp(jnp.where(allowed, logits, -jnp.inf))
            total = total + jnp.sum(weights, axis=-1)
            weighted = weighted + jnp.einsum(
                "cgts,scd->cgtd",
                weights.astype(jnp.bfloat16),
                value_block,
                preferred_element_type=jnp.float32,
            )
            return (weighted, total)

        def skipped(state):
            return state

        return lax.cond(first <= last_row, compute, skipped, inner)

    weighted, total = lax.fori_loop(0, count, one_block, init)
    result = weighted / total[..., None]
    attended = (
        jnp.transpose(result, (2, 0, 1, 3)).reshape(tok_dev, gate_heads * HEAD).astype(jnp.bfloat16)
    )
    out_ret, out_att = (
        lax.all_gather(w_out_ret, "sp", axis=1, tiled=True),
        lax.all_gather(w_out_att, "sp", axis=1, tiled=True),
    )
    return lax.psum_scatter(
        (
            jnp.dot(retained, out_ret, preferred_element_type=jnp.float32)
            + jnp.dot(attended, out_att, preferred_element_type=jnp.float32)
        ).astype(jnp.bfloat16),
        "tp",
        scatter_dimension=0,
        tiled=True,
    )


def choose(n, m, *arrays):
    tokens, w_key_ret, w_out_ret = arrays[0], arrays[3], arrays[8]
    whole_tiles = w_out_ret.shape[1] % LANES == 0 and w_key_ret.shape[0] % LANES == 0
    heads = arrays[10].shape[1]
    small = 16 * heads <= HEAD and arrays[7].shape[1] == HEAD and arrays[11].shape[0] == heads
    if whole_tiles and small and tokens.shape[0] * m == SPAN:
        return body(n, m, *arrays)
    return plain_body(*arrays)


def solution(mesh):
    return jax.shard_map(
        functools.partial(choose, mesh.shape["sp"], mesh.shape["tp"]),
        mesh=mesh,
        in_specs=(
            P(("sp", "tp"), None),
            P(),
            P("sp", "tp"),
            P("sp", "tp"),
            P("sp", "tp"),
            P("sp", "tp"),
            P("sp", "tp"),
            P("sp", "tp"),
            P("tp", "sp"),
            P("tp", "sp"),
            P("sp", "tp"),
            P("tp", None),
        ),
        out_specs=P(("sp", "tp"), None),
        check_vma=False,
    )
```

```python
import functools

import jax
import jax.numpy as jnp
import numpy as np
from jax import lax
from jax.experimental import pallas as pl
from jax.experimental.pallas import tpu as pltpu
from jax.sharding import PartitionSpec as P

HEAD = 64
EPS = 1e-06
THETA = 10000.0
F32 = jnp.float32
BF16 = jnp.bfloat16
MESH = pl.DeviceIdType.MESH
SPAN = 256
KEY_SPAN = 256
LANES = 128
CHUNKS = (4, 4, 4, 2)
HIGH = lax.Precision.HIGHEST


def ring_to_sp(place, n):
    if n % 2:
        return place
    back = place // (n // 2)
    return (1 - back) * 2 * place + back * (2 * (n - 1 - place) + 1)


def sp_to_ring(index, n):
    if n % 2:
        return index
    odd, pair = index % 2, index // 2
    return (1 - odd) * pair + odd * (n - 1 - pair)


def dot(a, b, dims=((1,), (0,))):
    return lax.dot_general(a, b, (dims, ((), ())), preferred_element_type=F32)


def kernel(
    n,
    m,
    heads,
    chunks,
    tok_hbm,
    gain_ref,
    wq_ret_hbm,
    wk_ret_hbm,
    wv_ret_hbm,
    wq_att_hbm,
    wk_att_hbm,
    wv_att_hbm,
    wo_ret_hbm,
    wo_att_hbm,
    table_hbm,
    logs_ref,
    gate_ref,
    out_ref,
    tokens,
    table,
    xbuf,
    abuf,
    bbuf,
    obuf,
    kvbuf,
    state,
    num,
    den,
    outbuf,
    rsbuf,
    *sems,
):
    (load, x_send, x_recv, a_send, a_recv, b_send, b_recv, o_send, o_recv, k_send, k_recv, r_send,
     r_recv) = sems
    me = lax.axis_index("sp")
    mine = lax.axis_index("tp")
    place = sp_to_ring(me, n)
    right = ring_to_sp((place + 1) % n, n)
    left = ring_to_sp((place + n - 1) % n, n)
    tok = xbuf.shape[0]
    rows = tok // m
    width = heads * HEAD

    half_o = wo_ret_hbm.shape[0]
    loads = [
        pltpu.make_async_copy(source, target, load.at[k])
        for k, (source, target) in enumerate((
            (wk_att_hbm, abuf.at[me, pl.ds(0, HEAD)]),
            (wv_att_hbm, abuf.at[me, pl.ds(HEAD, HEAD)]),
            (wk_ret_hbm, abuf.at[me, pl.ds(2 * HEAD, width)]),
            (wv_ret_hbm, abuf.at[me, pl.ds(2 * HEAD + width, width)]),
            (tok_hbm, tokens),
            (wq_att_hbm, bbuf.at[me, pl.ds(0, width)]),
            (wq_ret_hbm, bbuf.at[me, pl.ds(width, width)]),
            (table_hbm.at[pl.ds(pl.multiple_of(me * tok, tok), tok)], table),
            (wo_ret_hbm, obuf.at[me, pl.ds(0, half_o)]),
            (wo_att_hbm, obuf.at[me, pl.ds(half_o, wo_att_hbm.shape[0])]),
        ))
    ]
    for copy in loads:
        copy.start()

    barrier = pltpu.get_barrier_semaphore()
    for other in (left, right):
        pl.semaphore_signal(barrier, inc=1, device_id={"sp": other}, device_id_type=MESH)
    for r in range(1, m):
        pl.semaphore_signal(barrier, inc=1, device_id={"tp": (mine + r) % m}, device_id_type=MESH)

    for copy in loads[:4]:
        copy.wait()
    pl.semaphore_wait(barrier, 2 + m - 1)

    rounds = n // 2
    full = (n - 1) // 2

    def ring_copy(buf, send, recv, pieces, step, way, chunk, arriving):
        hops = step + 1 if arriving else step
        owner = ring_to_sp((place + (n - hops if way == 0 else hops)) % n, n)
        piece = buf.shape[1] // pieces
        span = pl.ds(chunk * piece, piece)
        return pltpu.make_async_remote_copy(
            src_ref=buf.at[owner, span],
            dst_ref=buf.at[owner, span],
            send_sem=send.at[way, step, chunk],
            recv_sem=recv.at[way, step, chunk],
            device_id={"sp": right if way == 0 else left},
            device_id_type=MESH,
        )

    started = []

    def travels(pieces, step, way, chunk):
        if step < full:
            return True
        return step < rounds and (chunk < pieces // 2) == (way == 0)

    def ring_step(group, step):
        for chunk in range(group[3]):
            for way in range(2):
                if step > 0 and travels(group[3], step - 1, way, chunk):
                    ring_copy(*group, step - 1, way, chunk, True).wait_recv()
                if travels(group[3], step, way, chunk):
                    copy = ring_copy(*group, step, way, chunk, False)
                    copy.start()
                    started.append(copy)

    ring_a = (abuf, a_send, a_recv, chunks[0])
    ring_b = (bbuf, b_send, b_recv, chunks[1])
    ring_o = (obuf, o_send, o_recv, chunks[2])
    ring_k = (kvbuf, k_send, k_recv, chunks[3])

    ring_step(ring_a, 0)
    loads[4].wait()
    values = tokens[...].astype(F32)
    scale = lax.rsqrt(jnp.mean(values * values, axis=-1, keepdims=True) + EPS)
    own = pl.ds(mine * rows, rows)
    xbuf[own, :] = (values * scale * gain_ref[...]).astype(BF16)
    for r in range(1, m):
        copy = pltpu.make_async_remote_copy(
            src_ref=xbuf.at[own],
            dst_ref=xbuf.at[own],
            send_sem=x_send.at[r - 1],
            recv_sem=x_recv.at[r - 1],
            device_id={"tp": (mine + r) % m},
            device_id_type=MESH,
        )
        copy.start()
        started.append(copy)
    for copy in loads[5:]:
        copy.wait()
    lines = lax.broadcasted_iota(jnp.int32, (tok, tok), 0)
    across = lax.broadcasted_iota(jnp.int32, (tok, tok), 1)
    causal = lines >= across
    upto = jnp.where(lines <= across, 1.0, 0.0)
    logs = jnp.concatenate([logs_ref[...], jnp.zeros((8 - heads, tok), F32)], axis=0)
    turned = lax.dot_general(
        logs, upto, (((1,), (0,)), ((), ())),
        preferred_element_type=F32, precision=lax.Precision.HIGHEST,
    )
    fill = jnp.zeros((LANES - 8, tok), F32)
    within = jnp.concatenate([turned, fill], axis=0).T
    gates_own = gate_ref[:, pl.ds(pl.multiple_of(me * tok, tok), tok)]
    gate_col = jnp.concatenate(
        [gates_own, jnp.zeros((LANES - heads, tok), F32)], axis=0
    ).T
    cosine, sine = table[:, : HEAD // 2], table[:, HEAD // 2 :]

    for step in range(1, rounds):
        ring_step(ring_a, step)
    ring_step(ring_b, 0)
    for r in range(1, m):
        other = pl.ds(((mine + m - r) % m) * rows, rows)
        pltpu.make_async_remote_copy(
            src_ref=xbuf.at[other],
            dst_ref=xbuf.at[other],
            send_sem=x_send.at[r - 1],
            recv_sem=x_recv.at[r - 1],
            device_id={"tp": (mine + r) % m},
            device_id_type=MESH,
        ).wait_recv()
    ring_step(ring_a, rounds)
    ring_step(ring_b, 1)

    def rope(field):
        half = HEAD // 2
        first, second = field[:, :half], field[:, half:]
        return jnp.concatenate(
            [first * cosine - second * sine, first * sine + second * cosine], axis=-1
        )

    def project(buf):
        deep = buf.shape[2]
        return sum(
            dot(xbuf[:, k * deep : (k + 1) * deep], buf[k], ((1,), (1,))) for k in range(n)
        )

    proj = project(abuf)
    pair = proj[:, : 2 * HEAD].astype(BF16)
    keys, vals, updates, marks = [], [], [], []
    for h in range(heads):
        base = 2 * HEAD + h * HEAD
        key = rope(proj[:, base : base + HEAD]).astype(BF16)
        val = proj[:, base + width : base + width + HEAD].astype(BF16)
        column = within[:, h : h + 1]
        last = column[tok - 1 :, :]
        faded = (key.astype(F32) * jnp.exp(last - column)).astype(BF16)
        updates.append(dot(faded, val, ((0,), (0,))))
        high = last.astype(BF16).astype(F32)
        low = last - high
        marks.append(jnp.broadcast_to(high, (8, HEAD)))
        marks.append(jnp.broadcast_to(low, (8, HEAD)))
        keys.append(key)
        vals.append(val)
    kvbuf[me, :tok, :] = pair
    marks.append(jnp.zeros((HEAD - 16 * heads, HEAD), F32))
    blocks = updates + [jnp.concatenate(marks, axis=0)]
    if len(blocks) % 2:
        blocks.append(jnp.zeros((HEAD, HEAD), F32))
    for k in range(0, len(blocks), 2):
        both = jnp.concatenate(blocks[k : k + 2], axis=1).astype(BF16)
        kvbuf[me, tok + k // 2 * HEAD : tok + (k // 2 + 1) * HEAD, :] = both

    def piece_of(index, k):
        lanes = slice(k % 2 * HEAD, (k % 2 + 1) * HEAD)
        return kvbuf[index, tok + k // 2 * HEAD : tok + (k // 2 + 1) * HEAD, lanes].astype(F32)

    for step in range(rounds - 1):
        ring_step(ring_k, step)
        ring_step(ring_b, step + 2)
    ring_step(ring_k, rounds - 1)
    ring_step(ring_o, 0)

    projq = project(bbuf)
    ring_step(ring_k, rounds)
    ring_step(ring_o, 1)
    local, lifts = [], []
    for h in range(heads):
        base = width + h * HEAD
        query = (rope(projq[:, base : base + HEAD]) * HEAD ** (-0.5)).astype(BF16)
        column = within[:, h : h + 1]
        gap = jnp.where(causal, column - turned[h : h + 1, :], 0.0)
        scores = dot(query, keys[h], ((1,), (1,)))
        weights = jnp.where(causal, scores * jnp.exp(gap), 0.0).astype(BF16)
        local.append(dot(weights, vals[h]))
        lifts.append((query.astype(F32) * jnp.exp(column)).astype(BF16))

    queries = [
        (projq[:, h * HEAD : (h + 1) * HEAD] * HEAD ** (-0.5)).astype(BF16) for h in range(heads)
    ]

    def attend(index, masked):
        block = kvbuf[index, :tok, :]
        key, val = block[:, :HEAD], block[:, HEAD:]
        gates = gate_ref[:, pl.ds(pl.multiple_of(index * tok, tok), tok)]
        for h in range(heads):
            logits = dot(queries[h], key, ((1,), (1,)))
            logits = logits + gate_col[:, h : h + 1] - gates[h : h + 1, :]
            if masked:
                logits = jnp.where(causal, logits, -jnp.inf)
            weights = jnp.exp(logits)
            den[h] += jnp.broadcast_to(jnp.sum(weights, axis=-1, keepdims=True), (tok, HEAD))
            num[h] += dot(weights.astype(BF16), val)

    den[...] = jnp.zeros_like(den)
    num[...] = jnp.zeros_like(num)
    state[...] = jnp.zeros_like(state)
    attend(me, True)
    pending = list(range(2, rounds + 1))
    ring_step(ring_o, pending.pop(0))
    for j in range(n - 1):
        def earlier(j=j):
            marked = piece_of(j, heads)
            for h in range(heads):
                total = marked[16 * h : 16 * h + 1] + marked[16 * h + 8 : 16 * h + 9]
                state[h] = jnp.exp(total) * state[h] + piece_of(j, h)
            attend(j, False)

        pl.when(me > j)(earlier)
        if j % 3 == 2 and len(pending) > 1:
            ring_step(ring_o, pending.pop(0))
    for step in pending:
        ring_step(ring_o, step)

    retained, attended = [], []
    for h in range(heads):
        raw = local[h] + dot(lifts[h], state[h].astype(BF16))
        centre = jnp.mean(raw, axis=-1, keepdims=True)
        spread = jnp.mean(jnp.square(raw - centre), axis=-1, keepdims=True)
        retained.append(((raw - centre) * lax.rsqrt(spread + EPS)).astype(BF16))
        attended.append((num[h] / den[h]).astype(BF16))
    mixed = jnp.concatenate(retained + attended, axis=-1)

    def out_copy(r, part, span):
        return pltpu.make_async_remote_copy(
            src_ref=outbuf.at[(mine + r) % m, :, span],
            dst_ref=rsbuf.at[mine, :, span],
            send_sem=r_send.at[r - 1, part],
            recv_sem=r_recv.at[r - 1, part],
            device_id={"tp": (mine + r) % m},
            device_id_type=MESH,
        )

    columns = obuf.shape[2]
    group = 2 if n % 2 == 0 else 1
    for part in range(n // group):
        for k in range(part * group, part * group + group):
            share = dot(mixed, obuf[k]).astype(BF16)
            outbuf[:, :, k * columns : (k + 1) * columns] = share.reshape(m, rows, columns)
        span = pl.ds(part * group * columns, group * columns)
        for r in range(1, m):
            copy = out_copy(r, part, span)
            copy.start()
            started.append(copy)
    for part in range(n // group):
        span = pl.ds(part * group * columns, group * columns)
        total = outbuf[mine, :, span].astype(F32)
        for r in range(1, m):
            other = (mine + m - r) % m
            pltpu.make_async_remote_copy(
                src_ref=rsbuf.at[other, :, span],
                dst_ref=rsbuf.at[other, :, span],
                send_sem=r_send.at[r - 1, part],
                recv_sem=r_recv.at[r - 1, part],
                device_id={"tp": (mine + r) % m},
                device_id_type=MESH,
            ).wait_recv()
            total = total + rsbuf[other, :, span].astype(F32)
        out_ref[:, span] = total.astype(BF16)

    for copy in started:
        copy.wait_send()


def body(
    n,
    m,
    tokens,
    pre_gain,
    w_query_ret,
    w_key_ret,
    w_value_ret,
    w_query_att,
    w_key_att,
    w_value_att,
    w_out_ret,
    w_out_att,
    retain_log,
    forget_total,
):
    rows, depth = tokens.shape
    tok = rows * m
    heads = retain_log.shape[1]
    half = HEAD // 2
    inverse = np.float32(THETA) ** (-np.arange(half, dtype=np.float32) / np.float32(half))
    angles = np.arange(n * tok, dtype=np.float32)[:, None] * inverse[None, :]
    table = np.concatenate([np.cos(angles), np.sin(angles)], axis=1).astype(np.float32)
    chunks = CHUNKS
    wide_a = 2 * HEAD + 2 * heads * HEAD
    wide_b = 2 * heads * HEAD
    deep = w_key_ret.shape[0]
    deep_o = w_out_ret.shape[0] + w_out_att.shape[0]
    tall = tok + (heads // 2 + 1) * HEAD
    hbm = pl.BlockSpec(memory_space=pl.ANY)
    vmem = pl.BlockSpec(memory_space=pltpu.VMEM)
    dma = pltpu.SemaphoreType.DMA
    rings = [dma((2, n // 2, c)) for c in chunks for _ in range(2)]
    parts = n // 2 if n % 2 == 0 else n
    return pl.pallas_call(
        functools.partial(kernel, n, m, heads, chunks),
        out_shape=jax.ShapeDtypeStruct((rows, depth), BF16),
        in_specs=[hbm, vmem] + [hbm] * 9 + [vmem] * 2,
        out_specs=vmem,
        scratch_shapes=[
            pltpu.VMEM(tokens.shape, BF16),
            pltpu.VMEM((tok, HEAD), F32),
            pltpu.VMEM((tok, depth), BF16),
            pltpu.VMEM((n, wide_a, deep), BF16),
            pltpu.VMEM((n, wide_b, deep), BF16),
            pltpu.VMEM((n, deep_o, w_out_ret.shape[1]), BF16),
            pltpu.VMEM((n, tall, 2 * HEAD), BF16),
            pltpu.VMEM((heads, HEAD, HEAD), F32),
            pltpu.VMEM((heads, tok, HEAD), F32),
            pltpu.VMEM((heads, tok, HEAD), F32),
            pltpu.VMEM((m, rows, depth), BF16),
            pltpu.VMEM((m, rows, depth), BF16),
            dma((10,)),
            dma((m - 1,)),
            dma((m - 1,)),
            *rings,
            dma((m - 1, parts)),
            dma((m - 1, parts)),
        ],
        compiler_params=pltpu.CompilerParams(
            collective_id=0, has_side_effects=True, vmem_limit_bytes=60 * 1024 * 1024
        ),
    )(
        tokens,
        pre_gain[None, :],
        w_query_ret.T,
        w_key_ret.T,
        w_value_ret.T,
        w_query_att.T,
        w_key_att.T,
        w_value_att.T,
        w_out_ret,
        w_out_att,
        jnp.asarray(table),
        retain_log.T,
        forget_total,
    )


def rotate(field, positions):
    half = field.shape[-1] // 2
    inverse = THETA ** (-jnp.arange(half, dtype=jnp.float32) / half)
    angles = positions[:, None] * inverse[None, :]
    cosine = jnp.cos(angles)[:, None, :]
    sine = jnp.sin(angles)[:, None, :]
    first_half = field[..., :half]
    second_half = field[..., half:]
    return jnp.concatenate(
        [first_half * cosine - second_half * sine, first_half * sine + second_half * cosine],
        axis=-1,
    )


def head_norm(values):
    centre = jnp.mean(values, axis=-1, keepdims=True)
    spread = jnp.mean(jnp.square(values - centre), axis=-1, keepdims=True)
    return (values - centre) * lax.rsqrt(spread + EPS)


def advance(state, pair):
    decay, update = pair
    return (jnp.exp(decay)[:, None, None] * state + update, state)


def plain_body(
    tokens,
    pre_gain,
    w_query_ret,
    w_key_ret,
    w_value_ret,
    w_query_att,
    w_key_att,
    w_value_att,
    w_out_ret,
    w_out_att,
    retain_log,
    forget_total,
):
    rows = tokens.astype(jnp.float32)
    normed = (
        rows * lax.rsqrt(jnp.mean(rows * rows, axis=-1, keepdims=True) + EPS) * pre_gain
    ).astype(jnp.bfloat16)
    gathered = lax.all_gather(normed, "tp", axis=0, tiled=True)
    tok_dev = gathered.shape[0]
    offset = lax.axis_index("sp") * tok_dev
    query_places = offset + jnp.arange(tok_dev, dtype=jnp.int32)
    positions = query_places.astype(jnp.float32)

    def blocked(values):
        return values.reshape((tok_dev // SPAN, SPAN) + values.shape[1:])

    pieces = (
        lax.all_gather(w_query_ret, "sp", axis=0, tiled=True),
        lax.all_gather(w_key_ret, "sp", axis=0, tiled=True),
        lax.all_gather(w_value_ret, "sp", axis=0, tiled=True),
        lax.all_gather(w_query_att, "sp", axis=0, tiled=True),
        lax.all_gather(w_key_att, "sp", axis=0, tiled=True),
        lax.all_gather(w_value_att, "sp", axis=0, tiled=True),
    )
    projected = tuple(
        (jnp.dot(gathered, piece, preferred_element_type=jnp.float32) for piece in pieces)
    )
    heads = retain_log.shape[1]
    shape = (tok_dev, heads, HEAD)
    query = blocked(
        (rotate(projected[0].reshape(shape), positions) * HEAD ** (-0.5)).astype(jnp.bfloat16)
    )
    key_rows = blocked(rotate(projected[1].reshape(shape), positions).astype(jnp.bfloat16))
    value_rows = blocked(projected[2].astype(jnp.bfloat16).reshape(shape))
    within = jnp.cumsum(blocked(retain_log), axis=1)
    causal = jnp.arange(SPAN)[:, None] >= jnp.arange(SPAN)[None, :]
    scores = jnp.einsum("bthd,bshd->bhts", query, key_rows, preferred_element_type=jnp.float32)
    turned = jnp.transpose(within, (0, 2, 1))
    gap = jnp.where(causal, turned[:, :, :, None] - turned[:, :, None, :], 0.0)
    weights = jnp.where(causal, scores * jnp.exp(gap), 0.0).astype(jnp.bfloat16)
    local = jnp.einsum("bhts,bshd->bthd", weights, value_rows, preferred_element_type=jnp.float32)
    last = within[:, -1]
    faded = (key_rows.astype(jnp.float32) * jnp.exp(last[:, None, :] - within)[..., None]).astype(
        jnp.bfloat16
    )
    updates = jnp.einsum("bshd,bshe->bhde", faded, value_rows, preferred_element_type=jnp.float32)
    zero_state = jnp.zeros((heads, HEAD, HEAD), jnp.float32)
    final, _ = lax.scan(advance, zero_state, (last, updates))
    decay_total = jnp.sum(last, axis=0)
    own_state = final.reshape(heads, HEAD * HEAD)
    every_total = lax.all_gather(
        decay_total[None].astype(jnp.bfloat16), "sp", axis=0, tiled=True
    ).astype(jnp.float32)
    every_state = lax.all_gather(
        own_state[None].astype(jnp.bfloat16), "sp", axis=0, tiled=True
    ).astype(jnp.float32)
    device_order = jnp.arange(every_total.shape[0], dtype=jnp.int32)[:, None]
    earlier = device_order < lax.axis_index("sp")
    before = jnp.sum(jnp.where(earlier, every_total, 0.0), axis=0)
    through = jnp.cumsum(every_total, axis=0)
    fading = jnp.where(earlier, jnp.exp(jnp.where(earlier, before[None, :] - through, 0.0)), 0.0)
    incoming = jnp.einsum("jh,jhe->he", fading, every_state, precision=HIGH)
    _, befores = lax.scan(advance, incoming.reshape(heads, HEAD, HEAD), (last, updates))
    lifted = (query.astype(jnp.float32) * jnp.exp(within)[..., None]).astype(jnp.bfloat16)
    carried = jnp.einsum(
        "bthd,bhde->bthe", lifted, befores.astype(jnp.bfloat16), preferred_element_type=jnp.float32
    )
    retained = (
        head_norm((local + carried).reshape(shape))
        .astype(jnp.bfloat16)
        .reshape(tok_dev, heads * HEAD)
    )
    raw_key = projected[4]
    gate_heads = forget_total.shape[0]
    kv_local = raw_key.shape[1] // HEAD
    group = gate_heads // kv_local
    query = (
        (projected[3] * HEAD ** (-0.5)).astype(jnp.bfloat16).reshape(tok_dev, kv_local, group, HEAD)
    )
    key_rows = raw_key.astype(jnp.bfloat16)
    value_rows = projected[5].astype(jnp.bfloat16)
    gate_rows = lax.dynamic_slice_in_dim(forget_total, offset, tok_dev, 1).reshape(
        kv_local, group, tok_dev
    )
    last_row = offset + tok_dev - 1
    init = (
        jnp.zeros((kv_local, group, tok_dev, HEAD), jnp.float32),
        jnp.zeros((kv_local, group, tok_dev), jnp.float32),
    )
    key_piece = lax.all_gather(key_rows, "sp", axis=0, tiled=True)
    value_piece = lax.all_gather(value_rows, "sp", axis=0, tiled=True)
    count = key_piece.shape[0] // KEY_SPAN

    def one_block(index, inner):
        first = index * KEY_SPAN

        def compute(state):
            weighted, total = state
            key_block = lax.dynamic_slice_in_dim(key_piece, index * KEY_SPAN, KEY_SPAN, 0).reshape(
                KEY_SPAN, kv_local, HEAD
            )
            value_block = lax.dynamic_slice_in_dim(
                value_piece, index * KEY_SPAN, KEY_SPAN, 0
            ).reshape(KEY_SPAN, kv_local, HEAD)
            gate_keys = lax.dynamic_slice_in_dim(forget_total, first, KEY_SPAN, 1).reshape(
                kv_local, group, KEY_SPAN
            )
            scores = jnp.einsum(
                "tcgd,scd->cgts", query, key_block, preferred_element_type=jnp.float32
            )
            logits = scores + gate_rows[:, :, :, None] - gate_keys[:, :, None, :]
            allowed = (first + jnp.arange(KEY_SPAN, dtype=jnp.int32))[None, :] <= query_places[
                :, None
            ]
            weights = jnp.exp(jnp.where(allowed, logits, -jnp.inf))
            total = total + jnp.sum(weights, axis=-1)
            weighted = weighted + jnp.einsum(
                "cgts,scd->cgtd",
                weights.astype(jnp.bfloat16),
                value_block,
                preferred_element_type=jnp.float32,
            )
            return (weighted, total)

        def skipped(state):
            return state

        return lax.cond(first <= last_row, compute, skipped, inner)

    weighted, total = lax.fori_loop(0, count, one_block, init)
    result = weighted / total[..., None]
    attended = (
        jnp.transpose(result, (2, 0, 1, 3)).reshape(tok_dev, gate_heads * HEAD).astype(jnp.bfloat16)
    )
    out_ret, out_att = (
        lax.all_gather(w_out_ret, "sp", axis=1, tiled=True),
        lax.all_gather(w_out_att, "sp", axis=1, tiled=True),
    )
    return lax.psum_scatter(
        (
            jnp.dot(retained, out_ret, preferred_element_type=jnp.float32)
            + jnp.dot(attended, out_att, preferred_element_type=jnp.float32)
        ).astype(jnp.bfloat16),
        "tp",
        scatter_dimension=0,
        tiled=True,
    )


def choose(n, m, *arrays):
    tokens, w_key_ret, w_out_ret = arrays[0], arrays[3], arrays[8]
    whole_tiles = w_out_ret.shape[1] % LANES == 0 and w_key_ret.shape[0] % LANES == 0
    heads = arrays[10].shape[1]
    small = 16 * heads <= HEAD and arrays[7].shape[1] == HEAD and arrays[11].shape[0] == heads
    if n % 2 == 0 and n > 2 and whole_tiles and small and tokens.shape[0] * m == SPAN:
        return body(n, m, *arrays)
    return plain_body(*arrays)


def solution(mesh):
    return jax.shard_map(
        functools.partial(choose, mesh.shape["sp"], mesh.shape["tp"]),
        mesh=mesh,
        in_specs=(
            P(("sp", "tp"), None),
            P(),
            P("sp", "tp"),
            P("sp", "tp"),
            P("sp", "tp"),
            P("sp", "tp"),
            P("sp", "tp"),
            P("sp", "tp"),
            P("tp", "sp"),
            P("tp", "sp"),
            P("sp", "tp"),
            P("tp", None),
        ),
        out_specs=P(("sp", "tp"), None),
        check_vma=False,
    )
```
